256 devices in a mesh: kv: 32 (over z, x), tp: 8 (over y, core).
Axes of the slice: x: 4, y: 4, z: 8, core: 2. Of those that a mesh axis runs over, the one named last changes fastest.
Arguments:
- tokens: bfloat16 [256, 4, 4096], P(None, None, 'kv')
- norm_gain: float32 [4096], replicated, may hold values from 0.1 to 1.9
- w_query: bfloat16 [4096, 4096], P('kv', 'tp'), may hold values from -0.09375 to 0.09375
- w_key: bfloat16 [4096, 4096], P('kv', 'tp'), may hold values from -0.09375 to 0.09375
- w_value: bfloat16 [4096, 4096], P('kv', 'tp'), may hold values from -0.09375 to 0.09375
- w_gate: bfloat16 [4096, 4096], P('kv', 'tp'), may hold values from -0.09375 to 0.09375
- w_decay: bfloat16 [4096, 32], replicated, may hold values from -0.09375 to 0.09375
- w_beta: bfloat16 [4096, 32], replicated, may hold values from -0.09375 to 0.09375
- decay_rate: float32 [32], replicated, may hold values from 0.02 to 3
- head_gain: float32 [128], replicated, may hold values from 0.1 to 1.9
- w_out: bfloat16 [4096, 4096], P('tp', 'kv'), may hold values from -0.09375 to 0.09375
- state: float32 [256, 32, 128, 128], P('kv', 'tp'), may hold values from -0.4 to 0.4
- prev_keys: bfloat16 [256, 32, 4, 128], P('kv', 'tp'), may hold values from -6 to 6
- prev_values: bfloat16 [256, 32, 4, 128], P('kv', 'tp'), may hold values from -6 to 6
- prev_log_decay: float32 [256, 32, 4], P('kv', 'tp'), may hold values from -0.7 to -0.02
- prev_beta: float32 [256, 32, 4], P('kv', 'tp'), may hold values from 0.1 to 0.9
- accepted: int32 [256], P('kv'), may hold values from 0 to 4
Outputs:
- mixed: bfloat16 [256, 4, 4096], P('tp', None, 'kv')
- carried: float32 [256, 32, 128, 128], P('kv', 'tp')
The draws below stay inside these ranges and needn't reach their ends.
All inputs are finite; a program needn't handle non-finite values.
Results may differ from the reference program's by a relative error of at most 0.0069.
Values may be sent and summed in bfloat16 or wider, within the bound.
A program may use at most 128 MiB of HBM per device.

```python
import math
import jax
import jax.numpy as jnp
from jax import lax

D = 4096
HEADS = 32
DK = 128
DV = 128
PROPS = 4
BATCH = 256


def draw_tokens(key, part):
    column = jnp.arange(D, dtype=jnp.float32)
    rising = jnp.exp(math.log(4.0) * column / D)
    values = jax.random.normal(key, (BATCH, PROPS, D), jnp.float32) * rising
    return values.astype(jnp.bfloat16)


def place_ends(result, own_key, least, top_value):
    spot = [jax.random.randint(jax.random.fold_in(own_key, axis), (), 0, length) for axis, length in enumerate(result.shape)]
    widest = result.shape.index(max(result.shape))
    next_to = spot[:widest] + [(spot[widest] + 1) % result.shape[widest]] + spot[widest + 1:]
    return result.at[tuple(spot)].set(least).at[tuple(next_to)].set(top_value)


def block_scale(key, extent, split, low, high):
    def one(dim, parts):
        steps = jax.random.uniform(jax.random.fold_in(jax.random.fold_in(key, 6), dim), (parts,), jnp.float32, low / len(split), high / len(split))
        return jnp.repeat(jnp.exp(steps), extent[dim] // parts).reshape((-1,) + (1,) * (len(extent) - dim - 1))

    factor_of = one(*split[0])
    for cut in split[1:]:
        factor_of = factor_of * one(*cut)
    return factor_of


def scatter_about(key, extent, spread, limit, cuts=(), held_as=jnp.bfloat16):
    drawn = jax.random.normal(key, extent, jnp.float32) * spread
    if len(cuts) > 0:
        drawn = block_scale(key, extent, cuts, -0.22, 0.18) * drawn
    return jnp.clip(drawn, min=-limit, max=limit).astype(held_as)


def setup_inputs(seed: int = 0) -> dict:
    keys = jax.random.split(jax.random.key(seed), 18)
    return {
        "tokens": draw_tokens(jax.random.fold_in(keys[17], 71), 0),
        "norm_gain": jnp.clip(1.0 + 0.18 * jax.random.normal(keys[1], (D,), jnp.float32), 0.1, 1.9),
        "w_query": scatter_about(keys[2], (D, HEADS * DK), D ** -0.5, 0.09375, ((0, 32), (1, 8))),
        "w_key": scatter_about(keys[3], (D, HEADS * DK), D ** -0.5, 0.09375, ((0, 32), (1, 8))),
        "w_value": scatter_about(keys[4], (D, HEADS * DV), D ** -0.5, 0.09375, ((0, 32), (1, 8))),
        "w_gate": scatter_about(keys[5], (D, HEADS * DV), D ** -0.5, 0.09375, ((0, 32), (1, 8))),
        "w_decay": scatter_about(keys[6], (D, HEADS), D ** -0.5, 0.09375),
        "w_beta": scatter_about(keys[7], (D, HEADS), D ** -0.5, 0.09375),
        "decay_rate": jnp.clip(jnp.exp(jax.random.uniform(keys[8], (HEADS,), jnp.float32, math.log(0.02), math.log(3.0))), 0.02, 3.0),
        "head_gain": jnp.clip(1.0 + 0.18 * jax.random.normal(keys[9], (DV,), jnp.float32), 0.1, 1.9),
        "w_out": scatter_about(keys[10], (HEADS * DV, D), (HEADS * DV) ** -0.5, 0.09375, ((0, 8), (1, 32))),
        "state": scatter_about(keys[11], (BATCH, HEADS, DK, DV), 0.05, 0.4, ((0, 32), (1, 8)), jnp.float32),
        "prev_keys": scatter_about(keys[12], (BATCH, HEADS, PROPS, DK), 1.0, 6.0, ((0, 32), (1, 8))),
        "prev_values": scatter_about(keys[13], (BATCH, HEADS, PROPS, DV), 1.0, 6.0, ((0, 32), (1, 8))),
        "prev_log_decay": jnp.clip(-0.7 + 0.68 * jax.random.uniform(keys[14], (BATCH, HEADS, PROPS), jnp.float32) ** block_scale(keys[14], (BATCH, HEADS, PROPS), ((0, 32), (1, 8)), -0.2, 0.2), -0.7, -0.02),
        "prev_beta": jnp.clip(0.1 + 0.79999997 * jax.random.uniform(keys[15], (BATCH, HEADS, PROPS), jnp.float32) ** block_scale(keys[15], (BATCH, HEADS, PROPS), ((0, 32), (1, 8)), -0.2, 0.2), 0.1, 0.9),
        "accepted": place_ends(jax.random.randint(keys[16], (BATCH,), 0, PROPS + 1), jax.random.fold_in(keys[16], 1), 0, PROPS).astype(jnp.int32),
    }


epsilon = 1e-06

def unit_rows(values):
    return values * lax.rsqrt(lax.optimization_barrier(jnp.sum(values * values, axis=-1, keepdims=True)) + epsilon)

def apply_update(matrix, keyvec, valvec, logd, strength):
    decayed = jnp.exp(logd)[..., None, None] * matrix
    predicted = jnp.einsum('bhde,bhd->bhe', decayed, keyvec, precision=lax.Precision.HIGHEST)
    change = strength[..., None] * (valvec - predicted)
    return decayed + jnp.einsum('bhd,bhe->bhde', keyvec, change, precision=lax.Precision.HIGHEST)

def reference(tokens, norm_gain, w_query, w_key, w_value, w_gate, w_decay, w_beta, decay_rate, head_gain, w_out, state, prev_keys, prev_values, prev_log_decay, prev_beta, accepted):
    f32 = jnp.float32
    rowsx = tokens.astype(f32).reshape(BATCH * PROPS, D)
    scale = lax.rsqrt(lax.optimization_barrier(jnp.mean(rowsx * rowsx, axis=1, keepdims=True)) + epsilon)
    normed = (rowsx * scale * norm_gain).astype(jnp.bfloat16)
    qraw = jnp.dot(normed, w_query, preferred_element_type=f32)
    kraw = jnp.dot(normed, w_key, preferred_element_type=f32)
    vraw = jnp.dot(normed, w_value, preferred_element_type=f32)
    zraw = jnp.dot(normed, w_gate, preferred_element_type=f32)
    araw = jnp.dot(normed, w_decay, preferred_element_type=f32)
    braw = jnp.dot(normed, w_beta, preferred_element_type=f32)
    query = unit_rows(jax.nn.silu(qraw).reshape(BATCH, PROPS, HEADS, DK)) * DK ** (-0.5)
    keyrow = unit_rows(jax.nn.silu(kraw).reshape(BATCH, PROPS, HEADS, DK))
    value = jax.nn.silu(vraw).reshape(BATCH, PROPS, HEADS, DV)
    beta = jax.nn.sigmoid(braw).reshape(BATCH, PROPS, HEADS)
    logdecay = (-decay_rate * jax.nn.softplus(araw)).reshape(BATCH, PROPS, HEADS)
    old_keys = unit_rows(prev_keys.astype(f32))
    old_values = prev_values.astype(f32)
    matrix = state
    for proposal in range(PROPS):
        keep = (proposal < accepted).astype(f32)[:, None]
        matrix = apply_update(matrix, old_keys[:, :, proposal], old_values[:, :, proposal], prev_log_decay[:, :, proposal] * keep, prev_beta[:, :, proposal] * keep)
    carried = matrix
    results = []
    for proposal in range(PROPS):
        matrix = apply_update(matrix, keyrow[:, proposal], value[:, proposal], logdecay[:, proposal], beta[:, proposal])
        results.append(jnp.einsum('bhde,bhd->bhe', matrix, query[:, proposal], precision=lax.Precision.HIGHEST))
    attended = jnp.stack(results, axis=1)
    zgate = zraw.reshape(BATCH, PROPS, HEADS, DV)
    headout = attended * lax.rsqrt(lax.optimization_barrier(jnp.mean(attended * attended, axis=-1, keepdims=True)) + epsilon)
    headout = (headout * head_gain * jax.nn.silu(zgate)).astype(jnp.bfloat16).reshape(BATCH * PROPS, HEADS * DV)
    mixed = jnp.dot(headout, w_out, preferred_element_type=f32).astype(jnp.bfloat16)
    return (mixed.reshape(BATCH, PROPS, D), carried)
```

```python
import jax
import jax.numpy as jnp
from jax import lax
from jax.experimental import pallas as pl
from jax.experimental.pallas import tpu as pltpu
from jax.sharding import PartitionSpec as P

MESH = pl.DeviceIdType.MESH
HIGHEST = lax.Precision.HIGHEST
epsilon = 1e-06

NZ, NX, NY, NT, NB, NH = 8, 4, 4, 4, 8, 4
f32, bf16 = jnp.float32, jnp.bfloat16


def contract(a, b, dims, precision=None):
    return lax.dot_general(a, b, (dims, ((), ())), precision=precision, preferred_element_type=f32)


def silu(v):
    return v / (1.0 + jnp.exp(-v))


def head(h):
    return slice(h * 128, (h + 1) * 128)


def across(v):
    return jnp.sum(v, axis=-1, keepdims=True)


def delta_rule(keys, predicted, values, logs, betas):
    decay = {}
    for t in range(NT):
        total = logs[t]
        decay[t, t] = None
        for i in range(t - 1, -1, -1):
            decay[t, i] = jnp.exp(total)
            total = total + logs[i]
        decay[t, -1] = jnp.exp(total)
    written = []
    for t in range(NT):
        expected = decay[t, -1] * predicted[t]
        for i in range(t):
            expected = expected + decay[t, i] * across(keys[i] * keys[t]) * written[i]
        written.append(betas[t] * (values[t] - expected))
    return written, decay


def kernel(
    tok, wkey, wquery, wvalue, wgate, wout, state, gain, abw, kold, vold, gold, bold, rate, hgain,
    mixed, carried,
    xtok, wbuf, stsend, strecv, scol, nbuf, absend, abrecv, yown, y1send, y1recv, y2send, y2recv,
    wobuf, sbuf, pbuf, ubuf, ebuf, tmp, kq, gnew, bnew, vnew, hout, hsend, hz, p3, d2d, rs2, yrecv, ofin, orecv,
    loc, ts, tr, wds, wdr, wrs, wrr, sts, str_, abs_, abr, y1s, y1r, y2s, y2r, wos, wor, hs, hr, ds_, dr, ys, yr, os_, or_,
):
    kv, tp = lax.axis_index("kv"), lax.axis_index("tp")
    z, x, y, c = kv // NX, lax.rem(kv, NX), tp // 2, lax.rem(tp, 2)
    side = 2 * lax.rem(z, 2) - 1
    weights = (wkey, wquery, wvalue, wgate)

    def at_z(zz):
        return {"kv": lax.rem(zz + 2 * NZ, NZ) * NX + x}

    def at_x(xx):
        return {"kv": z * NX + lax.rem(xx + NX, NX)}

    def at_y(yy):
        return {"tp": lax.rem(yy + NY, NY) * 2 + c}

    def dest(r):
        off = side * r if r < 4 else -side * (r - 3)
        return lax.rem(z + off + 2 * NZ, NZ)

    def remote(src, dst, send, recv, device):
        return pltpu.make_async_remote_copy(
            src_ref=src, dst_ref=dst, send_sem=send, recv_sem=recv, device_id=device, device_id_type=MESH
        )

    twin = {"tp": tp + 1 - 2 * c}
    pending = []

    def go(copy):
        copy.start()
        pending.append(copy)
        return copy

    own_tok = pltpu.make_async_copy(tok.at[:, x], xtok.at[0], loc.at[0])
    own_tok.start()
    own_w = [pltpu.make_async_copy(weights[m], wbuf.at[m, 0], loc.at[1 + m]) for m in range(4)]
    for copy in own_w:
        copy.start()
    own_s = pltpu.make_async_copy(state, sbuf, loc.at[5])
    own_s.start()
    own_wo = pltpu.make_async_copy(wout, wobuf.at[:, pl.ds(0, 128)], loc.at[6])
    own_wo.start()

    barrier = pltpu.get_barrier_semaphore()
    for d in range(1, NX):
        pl.semaphore_signal(barrier, inc=1, device_id=at_x(x + d), device_id_type=MESH)
    for d in range(1, NZ):
        pl.semaphore_signal(barrier, inc=1, device_id=at_z(z + d), device_id_type=MESH)
    for d in range(1, NY):
        pl.semaphore_signal(barrier, inc=1, device_id=at_y(y + d), device_id_type=MESH)
    pl.semaphore_signal(barrier, inc=1, device_id=twin, device_id_type=MESH)
    pl.semaphore_wait(barrier, NX + NZ + NY - 2)

    toks = [
        go(remote(tok.at[:, lax.rem(x + d, NX)], xtok.at[d], ts.at[d - 1], tr.at[d - 1], at_x(x + d)))
        for d in range(1, NX)
    ]

    def direct(m):
        return [
            go(remote(weights[m], wbuf.at[m, 1], wds.at[m, 0], wdr.at[m, 0], at_x(x + 1))),
            go(remote(weights[m], wbuf.at[m, 3], wds.at[m, 1], wdr.at[m, 1], at_x(x + 3))),
        ]

    def relay(m, copies):
        low, high = pl.ds(0, 64), pl.ds(64, 64)
        copies[0].wait_recv()
        first = go(remote(wbuf.at[m, 1, low], wbuf.at[m, 2, low], wrs.at[m, 0], wrr.at[m, 0], at_x(x + 1)))
        copies[1].wait_recv()
        second = go(remote(wbuf.at[m, 3, high], wbuf.at[m, 2, high], wrs.at[m, 1], wrr.at[m, 1], at_x(x + 3)))
        return [first, second]

    d0 = direct(0)
    d1 = direct(1)

    own_tok.wait()
    for copy in toks:
        copy.wait_recv()
    squares = jnp.zeros((NZ * 32, 128), f32)
    for d in range(NX):
        part = xtok[d].reshape(NZ * 32, 128).astype(f32)
        squares = squares + part * part
    stsend[...] = contract(jnp.ones((8, 128), f32), squares, ((1,), (1,)), HIGHEST)
    stats = [
        go(remote(stsend, strecv.at[d - 1], sts.at[d - 1], str_.at[d - 1], at_z(z + d))) for d in range(1, NZ)
    ]

    def products(left, b, h):
        rows = pl.ds(pl.multiple_of(b * 8, 8), 8)
        pbuf[h, rows] = contract(left[h, rows], sbuf[b * NH + h], ((1,), (0,)), HIGHEST)

    def all_products(left):
        @pl.loop(0, NB)
        def _(b):
            for h in range(NH):
                products(left, b, h)

    def every(ref, start, h):
        return ref[h, pl.ds(start, 8, stride=8)]

    own_s.wait()
    all_products(kold)

    r0 = relay(0, d0)
    d2 = direct(2)

    for copy in stats:
        copy.wait_recv()
    total = stsend[...]
    for d in range(NZ - 1):
        total = total + strecv[d]
    scale = lax.rsqrt(total * (1.0 / (NX * NZ * 128)) + epsilon)
    first_row = (lax.broadcasted_iota(jnp.int32, (8, 128), 0) == 0).astype(f32)
    scol[...] = contract(scale, first_row, ((0,), (0,)), HIGHEST).reshape(NZ, 32, 128)
    absend[...] = jnp.zeros((NZ, 8, 128), f32)
    for r in range(NZ):
        zz = dest(r)
        small = jnp.zeros((16, 32), f32)
        for d in range(NX):
            feature = lax.rem(x + NX - d, NX)
            normed = (xtok[d, zz].astype(f32) * scol[zz] * gain[feature]).astype(bf16)
            nbuf[r * 32 : (r + 1) * 32, head(d)] = normed
            small = small + contract(abw[feature], normed, ((1,), (1,)))
        absend[r, :, 0:32] = small[0:8]
    ab = [
        go(remote(absend.at[r], abrecv.at[r - 1], abs_.at[r - 1], abr.at[r - 1], at_z(dest(r))))
        for r in range(1, NZ)
    ]

    def project(m, copies):
        own_w[m].wait()
        for copy in copies:
            copy.wait_recv()
        rows = jnp.dot(nbuf[...], wbuf[m].reshape(512, 512), preferred_element_type=f32)
        yown[m] = rows[0:128]
        y1send[m] = rows[128:256].astype(bf16)
        return go(remote(y1send.at[m], y1recv.at[m], y1s.at[m], y1r.at[m], at_z(z + (-side))))

    def second_sum(m, copy):
        copy.wait_recv()
        rows = yown[m] + y1recv[m].astype(f32)
        yown[m, 0:32] = rows[0:32]
        y2send[m] = rows[32:128].astype(bf16).reshape(3, 32, 512)
        return [
            go(remote(y2send.at[m, i - 1], y2recv.at[m, i - 1], y2s.at[m, i - 1], y2r.at[m, i - 1], at_z(dest(i))))
            for i in (3, 2, 1)
        ]

    def summed(m, copies, lanes):
        rows = yown[m, 0:32, lanes]
        for i in range(3):
            rows = rows + y2recv[m, i, :, lanes].astype(f32)
        return rows

    y1_0 = project(0, r0)
    r1 = relay(1, d1)
    d3 = direct(3)

    for h in range(NH):
        keys = [every(kold, t, h) for t in range(NT)]
        written, decay = delta_rule(
            keys,
            [every(pbuf, t, h) for t in range(NT)],
            [vold[t, :, head(h)] for t in range(NT)],
            [gold[t, :, head(h)] for t in range(NT)],
            [bold[t, :, head(h)] for t in range(NT)],
        )
        for t in range(NT):
            last = written[t] if t == NT - 1 else decay[NT - 1, t] * written[t]
            ubuf[h, pl.ds(t, 8, stride=8)] = last
            ubuf[h, pl.ds(t + 4, 8, stride=8)] = jnp.zeros((8, 128), f32)
        ebuf[h, pl.ds(0, 8, stride=8)] = decay[NT - 1, -1]

    y2_0 = second_sum(0, y1_0)
    y1_1 = project(1, r1)
    r2 = relay(2, d2)
    wos_ = [
        go(remote(wout, wobuf.at[:, pl.ds(d * 128, 128)], wos.at[d - 1], wor.at[d - 1], at_x(x + d)))
        for d in range(1, NX)
    ]

    @pl.loop(0, NB)
    def _(b):
        rows = pl.ds(pl.multiple_of(b * 8, 8), 8)
        for h in range(NH):
            added = contract(kold[h, rows], ubuf[h, rows], ((0,), (0,)), HIGHEST)
            sbuf[b * NH + h] = sbuf[b * NH + h] * ebuf[h, rows][0:1] + added

    out_s = pltpu.make_async_copy(sbuf, carried, loc.at[7])
    out_s.start()

    y2_1 = second_sum(1, y1_1)
    y1_2 = project(2, r2)
    r3 = relay(3, d3)

    for copy in ab:
        copy.wait_recv()
    small = absend[0]
    for r in range(NZ - 1):
        small = small + abrecv[r]
    soft = jnp.maximum(small, 0.0) + jnp.log1p(jnp.exp(-jnp.abs(small)))
    which = lax.broadcasted_iota(jnp.int32, (8, 128), 0)
    small = jnp.where(which < NH, -rate[...] * soft, 1.0 / (1.0 + jnp.exp(-small)))
    row = lax.broadcasted_iota(jnp.int32, (8, 512), 0)
    lane = lax.broadcasted_iota(jnp.int32, (8, 512), 1) // 128
    logs = contract(small, (row == lane).astype(f32), ((0,), (0,)), HIGHEST)
    strengths = contract(small, (row == lane + NH).astype(f32), ((0,), (0,)), HIGHEST)
    for h in range(NH):
        gnew[h] = logs[0:32, head(h)]
        bnew[h] = strengths[0:32, head(h)]

    y1_3 = project(3, r3)
    y2_2 = second_sum(2, y1_2)

    def rows_of(ref, t, h):
        return ref[h, pl.ds(t, 8, stride=4)]

    for m, copies, factor in ((0, y2_0, 1.0), (1, y2_1, 128**-0.5)):
        for copy in copies:
            copy.wait_recv()
        for h in range(NH):
            v = silu(summed(m, copies, head(h)))
            tmp[h] = v * lax.rsqrt(across(v * v) + epsilon) * factor
            for t in range(NT):
                kq[h, pl.ds(m * 4 + t, 8, stride=8)] = rows_of(tmp, t, h)
    all_products(kq)

    y2_3 = second_sum(3, y1_3)
    for copy in y2_2:
        copy.wait_recv()
    for h in range(NH):
        vnew[h] = silu(summed(2, y2_2, head(h)))
    for h in range(NH):
        keys = [every(kq, t, h) for t in range(NT)]
        written, decay = delta_rule(
            keys,
            [every(pbuf, t, h) for t in range(NT)],
            [rows_of(vnew, t, h) for t in range(NT)],
            [rows_of(gnew, t, h) for t in range(NT)],
            [rows_of(bnew, t, h) for t in range(NT)],
        )
        for t in range(NT):
            query = every(kq, 4 + t, h)
            attended = decay[t, -1] * every(pbuf, 4 + t, h) + across(keys[t] * query) * written[t]
            for i in range(t):
                attended = attended + decay[t, i] * across(keys[i] * query) * written[i]
            scaled = attended * lax.rsqrt(across(attended * attended) * (1.0 / 128) + epsilon)
            hout[h, pl.ds(t, 8, stride=4)] = scaled * hgain[...]

    for copy in y2_3:
        copy.wait_recv()
    for h in range(NH):
        hsend[:, head(h)] = (hout[h] * silu(summed(3, y2_3, head(h)))).astype(bf16)
    heads = [go(remote(hsend, hz.at[d], hs.at[d - 1], hr.at[d - 1], at_z(z + d))) for d in (4, 3, 5, 2, 6, 1, 7)]
    hz[0] = hsend[...]

    own_wo.wait()
    for copy in wos_:
        copy.wait_recv()
    for copy in heads:
        copy.wait_recv()
    terms = jnp.dot(hz[...].reshape(256, 512), wobuf[...], preferred_element_type=f32)
    for d in range(NZ):
        zz = lax.rem(z + NZ - d, NZ)
        p3[lax.rem(zz, 2) * 4 + zz // 2] = terms[d * 32 : (d + 1) * 32]
    other = go(remote(p3.at[pl.ds((1 - c) * 4, 4)], d2d, ds_, dr, twin))
    other.wait_recv()
    for j in range(NY):
        rs2[j] = p3[c * 4 + j] + d2d[j]
    across_y = [
        go(remote(rs2.at[lax.rem(y + e, NY)], yrecv.at[e - 1], ys.at[e - 1], yr.at[e - 1], at_y(y + e)))
        for e in (2, 1, 3)
    ]
    for copy in across_y:
        copy.wait_recv()
    total = rs2[y]
    for e in range(NY - 1):
        total = total + yrecv[e]
    total = total.astype(bf16)
    for e in range(NX):
        ofin[e] = total[:, head(e)]
    outs = [
        go(remote(ofin.at[e], orecv.at[e - 1], os_.at[e - 1], or_.at[e - 1], at_x(x + NX - e)))
        for e in range(1, NX)
    ]
    mixed[x] = ofin[0]
    for e in range(1, NX):
        outs[e - 1].wait_recv()
        mixed[lax.rem(x + e, NX)] = orecv[e - 1]
    out_s.wait()
    for copy in pending:
        copy.wait_send()


def fused(*operands):
    anywhere = pl.BlockSpec(memory_space=pl.ANY)
    vmem = pl.BlockSpec(memory_space=pltpu.VMEM)
    dma = pltpu.SemaphoreType.DMA
    scratch = [
        pltpu.VMEM((NX, NZ, 32, 128), bf16),
        pltpu.VMEM((4, NX, 128, 512), bf16),
        pltpu.VMEM((8, 256), f32),
        pltpu.VMEM((NZ - 1, 8, 256), f32),
        pltpu.VMEM((NZ, 32, 128), f32),
        pltpu.VMEM((256, 512), bf16),
        pltpu.VMEM((NZ, 8, 128), f32),
        pltpu.VMEM((NZ - 1, 8, 128), f32),
        pltpu.VMEM((4, 128, 512), f32),
        pltpu.VMEM((4, 128, 512), bf16),
        pltpu.VMEM((4, 128, 512), bf16),
        pltpu.VMEM((4, 3, 32, 512), bf16),
        pltpu.VMEM((4, 3, 32, 512), bf16),
        pltpu.VMEM((512, 512), bf16),
        pltpu.VMEM((NB * NH, 128, 128), f32),
        pltpu.VMEM((NH, 64, 128), f32),
        pltpu.VMEM((NH, 64, 128), f32),
        pltpu.VMEM((NH, 64, 128), f32),
        pltpu.VMEM((NH, 32, 128), f32),
        pltpu.VMEM((NH, 64, 128), f32),
        pltpu.VMEM((NH, 32, 128), f32),
        pltpu.VMEM((NH, 32, 128), f32),
        pltpu.VMEM((NH, 32, 128), f32),
        pltpu.VMEM((NH, 32, 128), f32),
        pltpu.VMEM((32, 512), bf16),
        pltpu.VMEM((NZ, 32, 512), bf16),
        pltpu.VMEM((NZ, 32, 512), f32),
        pltpu.VMEM((NY, 32, 512), f32),
        pltpu.VMEM((NY, 32, 512), f32),
        pltpu.VMEM((NY - 1, 32, 512), f32),
        pltpu.VMEM((NX, 32, 128), bf16),
        pltpu.VMEM((NX - 1, 32, 128), bf16),
        dma((8,)),
        dma((3,)), dma((3,)),
        dma((4, 2)), dma((4, 2)), dma((4, 2)), dma((4, 2)),
        dma((7,)), dma((7,)), dma((7,)), dma((7,)),
        dma((4,)), dma((4,)), dma((4, 3)), dma((4, 3)),
        dma((3,)), dma((3,)),
        dma((7,)), dma((7,)),
        dma, dma,
        dma((3,)), dma((3,)), dma((3,)), dma((3,)),
    ]
    return pl.pallas_call(
        kernel,
        out_shape=(
            jax.ShapeDtypeStruct((NX, 32, 128), bf16),
            jax.ShapeDtypeStruct((NB * NH, 128, 128), f32),
        ),
        in_specs=[anywhere] * 7 + [vmem] * 8,
        out_specs=(vmem, anywhere),
        scratch_shapes=scratch,
        compiler_params=pltpu.CompilerParams(collective_id=0, has_side_effects=True),
        name="step",
    )(*operands)


def unit_rows(values):
    return values * lax.rsqrt(jnp.sum(values * values, axis=-1, keepdims=True) + epsilon)


def per_device(
    tokens,
    norm_gain,
    w_query,
    w_key,
    w_value,
    w_gate,
    w_decay,
    w_beta,
    decay_rate,
    head_gain,
    w_out,
    state,
    prev_keys,
    prev_values,
    prev_log_decay,
    prev_beta,
    accepted,
):
    z = lax.axis_index("kv") // NX
    head_start = lax.axis_index("tp") * NH
    gain = lax.dynamic_slice_in_dim(norm_gain, z * 512, 512, 0).reshape(NX, 1, 128)
    both = [lax.dynamic_slice(w, (z * 512, head_start), (512, NH)).T for w in (w_decay, w_beta)]
    abw = jnp.concatenate(both + [jnp.zeros((8, 512), bf16)], axis=0)
    abw = abw.reshape(16, NX, 128).transpose(1, 0, 2)
    rate = jnp.pad(lax.dynamic_slice_in_dim(decay_rate, head_start, NH, 0), (0, 4))
    rate = jnp.broadcast_to(rate[:, None], (8, 128))

    def by_step(v):
        return v.transpose(2, 0, 1, 3).reshape(NT, NB, NH * 128)

    kold = unit_rows(prev_keys.astype(f32)).transpose(1, 0, 2, 3)
    kold = jnp.pad(kold, ((0, 0), (0, 0), (0, 4), (0, 0))).reshape(NH, NB * 8, 128)
    vold = by_step(prev_values.astype(f32))
    keep = (jnp.arange(NT)[None, :] < accepted[:, None]).astype(f32)[:, None, :]
    wide = (NB, NH, NT, 128)
    gold = by_step(jnp.broadcast_to((prev_log_decay * keep)[..., None], wide))
    bold = by_step(jnp.broadcast_to((prev_beta * keep)[..., None], wide))
    mixed, carried = fused(
        tokens.reshape(NZ, NX, 32, 128), w_key, w_query, w_value, w_gate, w_out,
        state.reshape(NB * NH, 128, 128), gain, abw, kold, vold, gold, bold, rate, head_gain.reshape(1, 128),
    )
    return mixed.reshape(32, NT, 128), carried.reshape(NB, NH, 128, 128)


def solution(mesh):
    placed = (
        P(None, None, "kv"),
        P(),
        P("kv", "tp"),
        P("kv", "tp"),
        P("kv", "tp"),
        P("kv", "tp"),
        P(),
        P(),
        P(),
        P(),
        P("tp", "kv"),
        P("kv", "tp", None, None),
        P("kv", "tp", None, None),
        P("kv", "tp", None, None),
        P("kv", "tp", None),
        P("kv", "tp", None),
        P("kv"),
    )
    return jax.shard_map(
        per_device,
        mesh=mesh,
        in_specs=placed,
        out_specs=(P("tp", None, "kv"), P("kv", "tp", None, None)),
        check_vma=False,
    )
```

```python
import jax
import jax.numpy as jnp
from jax import lax
from jax.experimental import pallas as pl
from jax.experimental.pallas import tpu as pltpu
from jax.sharding import PartitionSpec as P

MESH = pl.DeviceIdType.MESH
HIGHEST = lax.Precision.HIGHEST
epsilon = 1e-06

NZ, NX, NY, NT, NB, NH = 8, 4, 4, 4, 8, 4
f32, bf16 = jnp.float32, jnp.bfloat16


def contract(a, b, dims, precision=None):
    return lax.dot_general(a, b, (dims, ((), ())), precision=precision, preferred_element_type=f32)


def silu(v):
    return v / (1.0 + jnp.exp(-v))


def head(h):
    return slice(h * 128, (h + 1) * 128)


def across(v):
    return jnp.sum(v, axis=-1, keepdims=True)


def delta_rule(keys, predicted, values, logs, betas):
    decay = {}
    for t in range(NT):
        total = logs[t]
        decay[t, t] = None
        for i in range(t - 1, -1, -1):
            decay[t, i] = jnp.exp(total)
            total = total + logs[i]
        decay[t, -1] = jnp.exp(total)
    written = []
    for t in range(NT):
        expected = decay[t, -1] * predicted[t]
        for i in range(t):
            expected = expected + decay[t, i] * across(keys[i] * keys[t]) * written[i]
        written.append(betas[t] * (values[t] - expected))
    return written, decay


def kernel(
    tok, wkey, wquery, wvalue, wgate, wout, state, *rest
):
    small_in, (mixed, sbuf, *rest) = rest[:10], rest[10:]
    small_ref, rest = rest[:10], rest[10:]
    gain, wdecay, wbeta, pkeys, pvalues, plogs, pbetas, accepted, rate, hgain = small_ref
    (
    small_sem, kraw, vraw, kold, gold, bold, abw, gainrow, xtok, wbuf, stsend, strecv, scol, nbuf, absend, abrecv, yown, y1send, y1recv, y2send, y2recv,
    wobuf, pbuf, ubuf, ebuf, tmp, kq, gnew, bnew, vnew, hout, hsend, hz, p3, d2d, rs2, yrecv, ofin, orecv,
    loc, ts, tr, wds, wdr, wrs, wrr, sts, str_, abs_, abr, y1s, y1r, y2s, y2r, wos, wor, hs, hr, ds_, dr, ys, yr, os_, or_,
    ) = rest
    kv, tp = lax.axis_index("kv"), lax.axis_index("tp")
    z, x, y, c = kv // NX, lax.rem(kv, NX), tp // 2, lax.rem(tp, 2)
    side = 2 * lax.rem(z, 2) - 1
    weights = (wkey, wquery, wvalue, wgate)

    def at_z(zz):
        return {"kv": lax.rem(zz + 2 * NZ, NZ) * NX + x}

    def at_x(xx):
        return {"kv": z * NX + lax.rem(xx + NX, NX)}

    def at_y(yy):
        return {"tp": lax.rem(yy + NY, NY) * 2 + c}

    def dest(r):
        off = side * r if r < 4 else -side * (r - 3)
        return lax.rem(z + off + 2 * NZ, NZ)

    def remote(src, dst, send, recv, device):
        return pltpu.make_async_remote_copy(
            src_ref=src, dst_ref=dst, send_sem=send, recv_sem=recv, device_id=device, device_id_type=MESH
        )

    twin = {"tp": tp + 1 - 2 * c}
    pending = []

    def go(copy):
        copy.start()
        pending.append(copy)
        return copy

    def arrive(name, *copies):
        with jax.named_scope(name):
            for copy in copies:
                copy.wait_recv()

    own_tok = pltpu.make_async_copy(tok.at[:, x], xtok.at[0], loc.at[0])
    own_tok.start()
    own_w = [pltpu.make_async_copy(weights[m], wbuf.at[m, 0], loc.at[1 + m]) for m in range(4)]
    for copy in own_w:
        copy.start()
    own_s = pltpu.make_async_copy(state, sbuf, loc.at[5])
    own_s.start()
    sources = list(small_in)
    for i in (1, 2):
        sources[i] = small_in[i].at[:, pl.ds(pl.multiple_of(z * 512, 512), 512)]
    own_small = [pltpu.make_async_copy(a, b, small_sem.at[i]) for i, (a, b) in enumerate(zip(sources, small_ref))]
    for copy in own_small:
        copy.start()
    own_wo = pltpu.make_async_copy(wout, wobuf.at[:, pl.ds(0, 128)], loc.at[6])
    own_wo.start()

    barrier = pltpu.get_barrier_semaphore()
    for d in range(1, NX):
        pl.semaphore_signal(barrier, inc=1, device_id=at_x(x + d), device_id_type=MESH)
    for d in range(1, NZ):
        pl.semaphore_signal(barrier, inc=1, device_id=at_z(z + d), device_id_type=MESH)
    for d in range(1, NY):
        pl.semaphore_signal(barrier, inc=1, device_id=at_y(y + d), device_id_type=MESH)
    pl.semaphore_signal(barrier, inc=1, device_id=twin, device_id_type=MESH)
    with jax.named_scope("barrier"):
        pl.semaphore_wait(barrier, NX + NZ + NY - 2)

    toks = [
        go(remote(tok.at[:, lax.rem(x + d, NX)], xtok.at[d], ts.at[d - 1], tr.at[d - 1], at_x(x + d)))
        for d in range(1, NX)
    ]

    def direct(m):
        return [
            go(remote(weights[m], wbuf.at[m, 1], wds.at[m, 0], wdr.at[m, 0], at_x(x + 1))),
            go(remote(weights[m], wbuf.at[m, 3], wds.at[m, 1], wdr.at[m, 1], at_x(x + 3))),
        ]

    def relay(m, copies):
        low, high = pl.ds(0, 64), pl.ds(64, 64)
        arrive(f"left{m}", copies[0])
        first = go(remote(wbuf.at[m, 1, low], wbuf.at[m, 2, low], wrs.at[m, 0], wrr.at[m, 0], at_x(x + 1)))
        arrive(f"right{m}", copies[1])
        second = go(remote(wbuf.at[m, 3, high], wbuf.at[m, 2, high], wrs.at[m, 1], wrr.at[m, 1], at_x(x + 3)))
        return [first, second]

    d0 = direct(0)
    d1 = direct(1)

    for copy in own_small:
        copy.wait()
    row = lax.broadcasted_iota(jnp.int32, (16, 32), 0)
    col = lax.broadcasted_iota(jnp.int32, (16, 32), 1) - tp * NH
    abw[...] = (
        contract(((row == col) & (row < NH)).astype(bf16), wdecay[...], ((1,), (0,)))
        + contract(((row == col + NH) & (row >= NH) & (row < 2 * NH)).astype(bf16), wbeta[...], ((1,), (0,)))
    ).astype(bf16)
    row = lax.broadcasted_iota(jnp.int32, (NX * NZ, 128), 0)
    for d in range(NX):
        here = row == z * NX + lax.rem(x + NX - d, NX)
        gainrow[d] = jnp.sum(jnp.where(here, gain[...], 0.0), axis=0, keepdims=True)
    keys = pkeys[...].astype(f32)
    kraw[...] = keys * lax.rsqrt(across(keys * keys) + epsilon)
    vraw[...] = pvalues[...].astype(f32)
    for h in range(NH):
        for t in range(NT):
            kold[h, pl.ds(t, 8, stride=8)] = kraw[pl.ds(h * NT + t, 8, stride=16)]
            kold[h, pl.ds(t + 4, 8, stride=8)] = jnp.zeros((8, 128), f32)
    kept = lax.rem(lax.broadcasted_iota(jnp.int32, (16, 8), 0), NT) < accepted[...]
    spread = lax.broadcasted_iota(jnp.int32, (16, 2048), 0) == lax.broadcasted_iota(jnp.int32, (16, 2048), 1) // 128
    spread = spread.astype(f32)
    gold[...] = contract(jnp.where(kept, plogs[...], 0.0), spread, ((0,), (0,)), HIGHEST)
    bold[...] = contract(jnp.where(kept, pbetas[...], 0.0), spread, ((0,), (0,)), HIGHEST)

    own_tok.wait()
    arrive("tokens", *toks)
    squares = jnp.zeros((NZ * 32, 128), f32)
    for d in range(NX):
        part = xtok[d].reshape(NZ * 32, 128).astype(f32)
        squares = squares + part * part
    stsend[...] = contract(jnp.ones((8, 128), f32), squares, ((1,), (1,)), HIGHEST)
    stats = [
        go(remote(stsend, strecv.at[d - 1], sts.at[d - 1], str_.at[d - 1], at_z(z + d))) for d in range(1, NZ)
    ]

    def products(left, b, h):
        rows = pl.ds(pl.multiple_of(b * 8, 8), 8)
        pbuf[h, rows] = contract(left[h, rows], sbuf[b * NH + h], ((1,), (0,)), HIGHEST)

    def all_products(left):
        @pl.loop(0, NB)
        def _(b):
            for h in range(NH):
                products(left, b, h)

    def every(ref, start, h):
        return ref[h, pl.ds(start, 8, stride=8)]

    own_s.wait()
    all_products(kold)

    r0 = relay(0, d0)
    d2 = direct(2)

    arrive("stats", *stats)
    total = stsend[...]
    for d in range(NZ - 1):
        total = total + strecv[d]
    scale = lax.rsqrt(total * (1.0 / (NX * NZ * 128)) + epsilon)
    first_row = (lax.broadcasted_iota(jnp.int32, (8, 128), 0) == 0).astype(f32)
    scol[...] = contract(scale, first_row, ((0,), (0,)), HIGHEST).reshape(NZ, 32, 128)
    absend[...] = jnp.zeros((NZ, 8, 128), f32)
    for r in range(NZ):
        zz = dest(r)
        small = jnp.zeros((16, 32), f32)
        for d in range(NX):
            feature = lax.rem(x + NX - d, NX)
            normed = (xtok[d, zz].astype(f32) * scol[zz] * gainrow[d]).astype(bf16)
            nbuf[r * 32 : (r + 1) * 32, head(d)] = normed
            small = small + contract(abw[:, pl.ds(pl.multiple_of(feature * 128, 128), 128)], normed, ((1,), (1,)))
        absend[r, :, 0:32] = small[0:8]
    ab = [
        go(remote(absend.at[r], abrecv.at[r - 1], abs_.at[r - 1], abr.at[r - 1], at_z(dest(r))))
        for r in range(1, NZ)
    ]

    def project(m, copies):
        own_w[m].wait()
        arrive(f"far{m}", *copies)
        rows = jnp.dot(nbuf[...], wbuf[m].reshape(512, 512), preferred_element_type=f32)
        yown[m] = rows[0:128]
        y1send[m] = rows[128:256].astype(bf16)
        return go(remote(y1send.at[m], y1recv.at[m], y1s.at[m], y1r.at[m], at_z(z + (-side))))

    def second_sum(m, copy):
        arrive(f"pair{m}", copy)
        rows = yown[m] + y1recv[m].astype(f32)
        yown[m, 0:32] = rows[0:32]
        y2send[m] = rows[32:128].astype(bf16).reshape(3, 32, 512)
        return [
            go(remote(y2send.at[m, i - 1], y2recv.at[m, i - 1], y2s.at[m, i - 1], y2r.at[m, i - 1], at_z(dest(i))))
            for i in (3, 2, 1)
        ]

    def summed(m, copies, lanes):
        rows = yown[m, 0:32, lanes]
        for i in range(3):
            rows = rows + y2recv[m, i, :, lanes].astype(f32)
        return rows

    y1_0 = project(0, r0)
    r1 = relay(1, d1)
    d3 = direct(3)

    for h in range(NH):
        keys = [every(kold, t, h) for t in range(NT)]
        written, decay = delta_rule(
            keys,
            [every(pbuf, t, h) for t in range(NT)],
            [vraw[pl.ds(h * NT + t, 8, stride=16)] for t in range(NT)],
            [gold[:, head(h * NT + t)] for t in range(NT)],
            [bold[:, head(h * NT + t)] for t in range(NT)],
        )
        for t in range(NT):
            last = written[t] if t == NT - 1 else decay[NT - 1, t] * written[t]
            ubuf[h, pl.ds(t, 8, stride=8)] = last
            ubuf[h, pl.ds(t + 4, 8, stride=8)] = jnp.zeros((8, 128), f32)
        ebuf[h, pl.ds(0, 8, stride=8)] = decay[NT - 1, -1]

    y2_0 = second_sum(0, y1_0)
    y1_1 = project(1, r1)
    r2 = relay(2, d2)
    wos_ = [
        go(remote(wout, wobuf.at[:, pl.ds(d * 128, 128)], wos.at[d - 1], wor.at[d - 1], at_x(x + d)))
        for d in range(1, NX)
    ]

    @pl.loop(0, NB)
    def _(b):
        rows = pl.ds(pl.multiple_of(b * 8, 8), 8)
        for h in range(NH):
            added = contract(kold[h, rows], ubuf[h, rows], ((0,), (0,)), HIGHEST)
            sbuf[b * NH + h] = sbuf[b * NH + h] * ebuf[h, rows][0:1] + added

    y2_1 = second_sum(1, y1_1)
    y1_2 = project(2, r2)
    r3 = relay(3, d3)

    arrive("small", *ab)
    small = absend[0]
    for r in range(NZ - 1):
        small = small + abrecv[r]
    soft = jnp.maximum(small, 0.0) + jnp.log1p(jnp.exp(-jnp.abs(small)))
    which = lax.broadcasted_iota(jnp.int32, (8, 128), 0)
    lane = lax.broadcasted_iota(jnp.int32, (8, 32), 1)
    mine = lane == tp * NH + lax.broadcasted_iota(jnp.int32, (8, 32), 0)
    rates = jnp.sum(jnp.where(mine, rate[...], 0.0), axis=1, keepdims=True)
    small = jnp.where(which < NH, -rates * soft, 1.0 / (1.0 + jnp.exp(-small)))
    row = lax.broadcasted_iota(jnp.int32, (8, 512), 0)
    lane = lax.broadcasted_iota(jnp.int32, (8, 512), 1) // 128
    logs = contract(small, (row == lane).astype(f32), ((0,), (0,)), HIGHEST)
    strengths = contract(small, (row == lane + NH).astype(f32), ((0,), (0,)), HIGHEST)
    for h in range(NH):
        gnew[h] = logs[0:32, head(h)]
        bnew[h] = strengths[0:32, head(h)]

    y1_3 = project(3, r3)
    y2_2 = second_sum(2, y1_2)

    def rows_of(ref, t, h):
        return ref[h, pl.ds(t, 8, stride=4)]

    for m, copies, factor in ((0, y2_0, 1.0), (1, y2_1, 128**-0.5)):
        arrive(f"sum{m}", *copies)
        for h in range(NH):
            v = silu(summed(m, copies, head(h)))
            tmp[h] = v * lax.rsqrt(across(v * v) + epsilon) * factor
            for t in range(NT):
                kq[h, pl.ds(m * 4 + t, 8, stride=8)] = rows_of(tmp, t, h)
    all_products(kq)

    y2_3 = second_sum(3, y1_3)
    arrive("sum2", *y2_2)
    for h in range(NH):
        vnew[h] = silu(summed(2, y2_2, head(h)))
    for h in range(NH):
        keys = [every(kq, t, h) for t in range(NT)]
        written, decay = delta_rule(
            keys,
            [every(pbuf, t, h) for t in range(NT)],
            [rows_of(vnew, t, h) for t in range(NT)],
            [rows_of(gnew, t, h) for t in range(NT)],
            [rows_of(bnew, t, h) for t in range(NT)],
        )
        for t in range(NT):
            query = every(kq, 4 + t, h)
            attended = decay[t, -1] * every(pbuf, 4 + t, h) + across(keys[t] * query) * written[t]
            for i in range(t):
                attended = attended + decay[t, i] * across(keys[i] * query) * written[i]
            scaled = attended * lax.rsqrt(across(attended * attended) * (1.0 / 128) + epsilon)
            hout[h, pl.ds(t, 8, stride=4)] = scaled * hgain[...]

    arrive("sum3", *y2_3)
    for h in range(NH):
        hsend[:, head(h)] = (hout[h] * silu(summed(3, y2_3, head(h)))).astype(bf16)
    heads = [go(remote(hsend, hz.at[d], hs.at[d - 1], hr.at[d - 1], at_z(z + d))) for d in (4, 3, 5, 2, 6, 1, 7)]
    hz[0] = hsend[...]

    own_wo.wait()
    arrive("wout", *wos_)
    arrive("heads", *heads)
    terms = jnp.dot(hz[...].reshape(256, 512), wobuf[...], preferred_element_type=f32)
    for d in range(NZ):
        zz = lax.rem(z + NZ - d, NZ)
        p3[lax.rem(zz, 2) * 4 + zz // 2] = terms[d * 32 : (d + 1) * 32]
    other = go(remote(p3.at[pl.ds((1 - c) * 4, 4)], d2d, ds_, dr, twin))
    arrive("twin", other)
    for j in range(NY):
        rs2[j] = p3[c * 4 + j] + d2d[j]
    across_y = [
        go(remote(rs2.at[lax.rem(y + e, NY)], yrecv.at[e - 1], ys.at[e - 1], yr.at[e - 1], at_y(y + e)))
        for e in (2, 1, 3)
    ]
    arrive("ysum", *across_y)
    total = rs2[y]
    for e in range(NY - 1):
        total = total + yrecv[e]
    total = total.astype(bf16)
    for e in range(NX):
        ofin[e] = total[:, head(e)]
    outs = [
        go(remote(ofin.at[e], orecv.at[e - 1], os_.at[e - 1], or_.at[e - 1], at_x(x + NX - e)))
        for e in range(1, NX)
    ]
    mixed[x] = ofin[0]
    arrive("outs", *outs)
    for e in range(1, NX):
        mixed[lax.rem(x + e, NX)] = orecv[e - 1]
    with jax.named_scope("drain"):
        for copy in pending:
            copy.wait_send()


def fused(*operands):
    anywhere = pl.BlockSpec(memory_space=pl.ANY)
    vmem = pl.BlockSpec(memory_space=pltpu.VMEM)
    dma = pltpu.SemaphoreType.DMA
    scratch = [
        pltpu.VMEM((NX * NZ, 128), f32),
        pltpu.VMEM((32, 512), bf16),
        pltpu.VMEM((32, 512), bf16),
        pltpu.VMEM((128, 128), bf16),
        pltpu.VMEM((128, 128), bf16),
        pltpu.VMEM((16, 8), f32),
        pltpu.VMEM((16, 8), f32),
        pltpu.VMEM((1, 8), jnp.int32),
        pltpu.VMEM((1, 32), f32),
        pltpu.VMEM((1, 128), f32),
        dma((10,)),
        pltpu.VMEM((128, 128), f32),
        pltpu.VMEM((128, 128), f32),
        pltpu.VMEM((NH, 64, 128), f32),
        pltpu.VMEM((8, 2048), f32),
        pltpu.VMEM((8, 2048), f32),
        pltpu.VMEM((16, 512), bf16),
        pltpu.VMEM((NX, 1, 128), f32),
        pltpu.VMEM((NX, NZ, 32, 128), bf16),
        pltpu.VMEM((4, NX, 128, 512), bf16),
        pltpu.VMEM((8, 256), f32),
        pltpu.VMEM((NZ - 1, 8, 256), f32),
        pltpu.VMEM((NZ, 32, 128), f32),
        pltpu.VMEM((256, 512), bf16),
        pltpu.VMEM((NZ, 8, 128), f32),
        pltpu.VMEM((NZ - 1, 8, 128), f32),
        pltpu.VMEM((4, 128, 512), f32),
        pltpu.VMEM((4, 128, 512), bf16),
        pltpu.VMEM((4, 128, 512), bf16),
        pltpu.VMEM((4, 3, 32, 512), bf16),
        pltpu.VMEM((4, 3, 32, 512), bf16),
        pltpu.VMEM((512, 512), bf16),
        pltpu.VMEM((NH, 64, 128), f32),
        pltpu.VMEM((NH, 64, 128), f32),
        pltpu.VMEM((NH, 64, 128), f32),
        pltpu.VMEM((NH, 32, 128), f32),
        pltpu.VMEM((NH, 64, 128), f32),
        pltpu.VMEM((NH, 32, 128), f32),
        pltpu.VMEM((NH, 32, 128), f32),
        pltpu.VMEM((NH, 32, 128), f32),
        pltpu.VMEM((NH, 32, 128), f32),
        pltpu.VMEM((32, 512), bf16),
        pltpu.VMEM((NZ, 32, 512), bf16),
        pltpu.VMEM((NZ, 32, 512), f32),
        pltpu.VMEM((NY, 32, 512), f32),
        pltpu.VMEM((NY, 32, 512), f32),
        pltpu.VMEM((NY - 1, 32, 512), f32),
        pltpu.VMEM((NX, 32, 128), bf16),
        pltpu.VMEM((NX - 1, 32, 128), bf16),
        dma((8,)),
        dma((3,)), dma((3,)),
        dma((4, 2)), dma((4, 2)), dma((4, 2)), dma((4, 2)),
        dma((7,)), dma((7,)), dma((7,)), dma((7,)),
        dma((4,)), dma((4,)), dma((4, 3)), dma((4, 3)),
        dma((3,)), dma((3,)),
        dma((7,)), dma((7,)),
        dma, dma,
        dma((3,)), dma((3,)), dma((3,)), dma((3,)),
    ]
    return pl.pallas_call(
        kernel,
        out_shape=(
            pltpu.VMEM((NX, 32, 128), bf16),
            pltpu.VMEM((NB * NH, 128, 128), f32),
        ),
        in_specs=[anywhere] * 17,
        out_specs=(vmem, vmem),
        scratch_shapes=scratch,
        compiler_params=pltpu.CompilerParams(collective_id=0, has_side_effects=True),
        name="step",
    )(*operands)


def per_device(
    tokens,
    norm_gain,
    w_query,
    w_key,
    w_value,
    w_gate,
    w_decay,
    w_beta,
    decay_rate,
    head_gain,
    w_out,
    state,
    prev_keys,
    prev_values,
    prev_log_decay,
    prev_beta,
    accepted,
):
    mixed, carried = fused(
        tokens.reshape(NZ, NX, 32, 128), w_key, w_query, w_value, w_gate, w_out,
        state.reshape(NB * NH, 128, 128), norm_gain.reshape(NX * NZ, 128), w_decay.T, w_beta.T,
        prev_keys.reshape(128, 128), prev_values.reshape(128, 128),
        prev_log_decay.transpose(1, 2, 0).reshape(16, NB), prev_beta.transpose(1, 2, 0).reshape(16, NB),
        accepted.reshape(1, NB), decay_rate.reshape(1, 32), head_gain.reshape(1, 128),
    )
    return mixed.reshape(32, NT, 128), carried.reshape(NB, NH, 128, 128)


def solution(mesh):
    placed = (
        P(None, None, "kv"),
        P(),
        P("kv", "tp"),
        P("kv", "tp"),
        P("kv", "tp"),
        P("kv", "tp"),
        P(),
        P(),
        P(),
        P(),
        P("tp", "kv"),
        P("kv", "tp", None, None),
        P("kv", "tp", None, None),
        P("kv", "tp", None, None),
        P("kv", "tp", None),
        P("kv", "tp", None),
        P("kv"),
    )
    return jax.shard_map(
        per_device,
        mesh=mesh,
        in_specs=placed,
        out_specs=(P("tp", None, "kv"), P("kv", "tp", None, None)),
        check_vma=False,
    )
```

```python
import jax
import jax.numpy as jnp
from jax import lax
from jax.experimental import pallas as pl
from jax.experimental.pallas import tpu as pltpu
from jax.sharding import PartitionSpec as P

MESH = pl.DeviceIdType.MESH
HIGHEST = lax.Precision.HIGHEST
epsilon = 1e-06

NZ, NX, NY, NT, NB, NH = 8, 4, 4, 4, 8, 4
f32, bf16 = jnp.float32, jnp.bfloat16


def contract(a, b, dims, precision=None):
    return lax.dot_general(a, b, (dims, ((), ())), precision=precision, preferred_element_type=f32)


def silu(v):
    return v / (1.0 + jnp.exp(-v))


def head(h):
    return slice(h * 128, (h + 1) * 128)


def across(v):
    return jnp.sum(v, axis=-1, keepdims=True)


def delta_rule(keys, predicted, values, logs, betas):
    decay = {}
    for t in range(NT):
        total = logs[t]
        decay[t, t] = None
        for i in range(t - 1, -1, -1):
            decay[t, i] = jnp.exp(total)
            total = total + logs[i]
        decay[t, -1] = jnp.exp(total)
    written = []
    for t in range(NT):
        expected = decay[t, -1] * predicted[t]
        for i in range(t):
            expected = expected + decay[t, i] * across(keys[i] * keys[t]) * written[i]
        written.append(betas[t] * (values[t] - expected))
    return written, decay


def kernel(
    tok, wkey, wquery, wvalue, wgate, wout, state, *rest
):
    small_in, (mixed, sbuf, *rest) = rest[:10], rest[10:]
    small_ref, rest = rest[:10], rest[10:]
    gain, wdecay, wbeta, pkeys, pvalues, plogs, pbetas, accepted, rate, hgain = small_ref
    (
    small_sem, kraw, vraw, kold, gold, bold, abw, gainrow, tokbuf, xtok, wbuf, stsend, strecv, scol, nbuf, absend, abrecv, yown, y1send, y1recv, y2send, y2recv,
    wobuf, pbuf, ubuf, ebuf, tmp, kq, gnew, bnew, vnew, hout, hsend, hz, p3, d2d, psend, precv,
    loc, ts, tr, wds, wdr, wrs, wrr, sts, str_, abs_, abr, y1s, y1r, y2s, y2r, wos, wor, hs, hr, tws, twr, ps, pr,
    ) = rest
    kv, tp = lax.axis_index("kv"), lax.axis_index("tp")
    z, x, y, c = kv // NX, lax.rem(kv, NX), tp // 2, lax.rem(tp, 2)
    side = 2 * lax.rem(z, 2) - 1
    weights = (wkey, wquery, wvalue, wgate)

    def at_z(zz):
        return {"kv": lax.rem(zz + 2 * NZ, NZ) * NX + x}

    def at_x(xx):
        return {"kv": z * NX + lax.rem(xx + NX, NX)}

    def dest(r):
        off = side * r if r < 4 else -side * (r - 3)
        return lax.rem(z + off + 2 * NZ, NZ)

    def remote(src, dst, send, recv, device):
        return pltpu.make_async_remote_copy(
            src_ref=src, dst_ref=dst, send_sem=send, recv_sem=recv, device_id=device, device_id_type=MESH
        )

    twin = {"tp": tp + 1 - 2 * c}
    pending = []

    def go(copy):
        copy.start()
        pending.append(copy)
        return copy

    def arrive(name, *copies):
        with jax.named_scope(name):
            for copy in copies:
                copy.wait_recv()

    own_tok = pltpu.make_async_copy(tok, tokbuf, loc.at[0])
    own_tok.start()
    own_w = [pltpu.make_async_copy(weights[m], wbuf.at[m, 0], loc.at[1 + m]) for m in range(4)]
    own_w[0].start()
    sources = list(small_in)
    for i in (1, 2):
        sources[i] = small_in[i].at[:, pl.ds(pl.multiple_of(z * 512, 512), 512)]
    own_small = [pltpu.make_async_copy(a, b, small_sem.at[i]) for i, (a, b) in enumerate(zip(sources, small_ref))]
    for copy in own_small:
        copy.start()
    own_s = pltpu.make_async_copy(state, sbuf, loc.at[5])
    own_s.start()
    for copy in own_w[1:]:
        copy.start()
    own_wo = pltpu.make_async_copy(wout, wobuf.at[:, pl.ds(0, 128)], loc.at[6])
    own_wo.start()

    barrier = pltpu.get_barrier_semaphore()
    for ey in range(NY):
        for ex in range(NX):
            if ey or ex:
                there = {"kv": z * NX + lax.rem(x + ex, NX), "tp": lax.rem(y + ey, NY) * 2 + c}
                pl.semaphore_signal(barrier, inc=1, device_id=there, device_id_type=MESH)
    for d in range(1, NZ):
        pl.semaphore_signal(barrier, inc=1, device_id=at_z(z + d), device_id_type=MESH)
    pl.semaphore_signal(barrier, inc=1, device_id=twin, device_id_type=MESH)

    for copy in own_small:
        copy.wait()
    row = lax.broadcasted_iota(jnp.int32, (16, 32), 0)
    col = lax.broadcasted_iota(jnp.int32, (16, 32), 1) - tp * NH
    abw[...] = (
        contract(((row == col) & (row < NH)).astype(bf16), wdecay[...], ((1,), (0,)))
        + contract(((row == col + NH) & (row >= NH) & (row < 2 * NH)).astype(bf16), wbeta[...], ((1,), (0,)))
    ).astype(bf16)
    row = lax.broadcasted_iota(jnp.int32, (NX * NZ, 128), 0)
    for d in range(NX):
        here = row == z * NX + lax.rem(x + NX - d, NX)
        gainrow[d] = jnp.sum(jnp.where(here, gain[...], 0.0), axis=0, keepdims=True)
    keys = pkeys[...].astype(f32)
    kraw[...] = keys * lax.rsqrt(across(keys * keys) + epsilon)
    vraw[...] = pvalues[...].astype(f32)
    for h in range(NH):
        for t in range(NT):
            kold[h, pl.ds(t, 8, stride=8)] = kraw[pl.ds(h * NT + t, 8, stride=16)]
            kold[h, pl.ds(t + 4, 8, stride=8)] = jnp.zeros((8, 128), f32)
    kept = lax.rem(lax.broadcasted_iota(jnp.int32, (16, 8), 0), NT) < accepted[...]
    spread = lax.broadcasted_iota(jnp.int32, (16, 2048), 0) == lax.broadcasted_iota(jnp.int32, (16, 2048), 1) // 128
    spread = spread.astype(f32)
    gold[...] = contract(jnp.where(kept, plogs[...], 0.0), spread, ((0,), (0,)), HIGHEST)
    bold[...] = contract(jnp.where(kept, pbetas[...], 0.0), spread, ((0,), (0,)), HIGHEST)
    own_tok.wait()
    own_w[0].wait()
    with jax.named_scope("barrier"):
        pl.semaphore_wait(barrier, NX * NY + NZ - 1)

    mine = pl.ds(c * 4, 4)
    toks = [
        go(remote(tokbuf.at[mine, lax.rem(x + d, NX)], xtok.at[d, mine], ts.at[d - 1], tr.at[d - 1], at_x(x + d)))
        for d in range(1, NX)
    ]

    def direct(m):
        return [
            go(remote(wbuf.at[m, 0], wbuf.at[m, 1], wds.at[m, 0], wdr.at[m, 0], at_x(x + 1))),
            go(remote(wbuf.at[m, 0], wbuf.at[m, 3], wds.at[m, 1], wdr.at[m, 1], at_x(x + 3))),
        ]

    def relay(m, copies):
        low, high = pl.ds(0, 64), pl.ds(64, 64)
        arrive(f"left{m}", copies[0])
        first = go(remote(wbuf.at[m, 1, low], wbuf.at[m, 2, low], wrs.at[m, 0], wrr.at[m, 0], at_x(x + 1)))
        arrive(f"right{m}", copies[1])
        second = go(remote(wbuf.at[m, 3, high], wbuf.at[m, 2, high], wrs.at[m, 1], wrr.at[m, 1], at_x(x + 3)))
        return [first, second]

    d0 = direct(0)
    own_w[1].wait()
    d1 = direct(1)

    def products(left, b, h):
        rows = pl.ds(pl.multiple_of(b * 8, 8), 8)
        pbuf[h, rows] = contract(left[h, rows], sbuf[b * NH + h], ((1,), (0,)), HIGHEST)

    def all_products(left, first, last):
        @pl.loop(first, last)
        def _(b):
            for h in range(NH):
                products(left, b, h)

    def every(ref, start, h):
        return ref[h, pl.ds(start, 8, stride=8)]

    def update_state(first, last):
        @pl.loop(first, last)
        def _(b):
            rows = pl.ds(pl.multiple_of(b * 8, 8), 8)
            for h in range(NH):
                added = contract(kold[h, rows], ubuf[h, rows], ((0,), (0,)), HIGHEST)
                sbuf[b * NH + h] = sbuf[b * NH + h] * ebuf[h, rows][0:1] + added

    own_s.wait()
    all_products(kold, 0, NB)

    shared = []
    for d in (1, 3, 2):
        arrive(f"tokens{d}", toks[d - 1])
        shared.append(
            go(remote(xtok.at[d, mine], xtok.at[d, mine], tws.at[d - 1], twr.at[d - 1], twin))
        )
    xtok[0] = tokbuf[:, x]
    arrive("tokens", *shared)
    squares = jnp.zeros((NZ * 32, 128), f32)
    for d in range(NX):
        part = xtok[d].reshape(NZ * 32, 128).astype(f32)
        squares = squares + part * part
    stsend[...] = contract(jnp.ones((8, 128), f32), squares, ((1,), (1,)), HIGHEST)
    stats = [
        go(remote(stsend, strecv.at[d - 1], sts.at[d - 1], str_.at[d - 1], at_z(z + d))) for d in (4, 3, 5, 2, 6, 1, 7)
    ]

    for h in range(NH):
        keys = [every(kold, t, h) for t in range(NT)]
        written, decay = delta_rule(
            keys,
            [every(pbuf, t, h) for t in range(NT)],
            [vraw[pl.ds(h * NT + t, 8, stride=16)] for t in range(NT)],
            [gold[:, head(h * NT + t)] for t in range(NT)],
            [bold[:, head(h * NT + t)] for t in range(NT)],
        )
        for t in range(NT):
            last = written[t] if t == NT - 1 else decay[NT - 1, t] * written[t]
            ubuf[h, pl.ds(t, 8, stride=8)] = last
            ubuf[h, pl.ds(t + 4, 8, stride=8)] = jnp.zeros((8, 128), f32)
        ebuf[h, pl.ds(0, 8, stride=8)] = decay[NT - 1, -1]
    update_state(0, 4)

    r0 = relay(0, d0)
    own_w[2].wait()
    d2 = direct(2)

    arrive("stats", *stats)
    total = stsend[...]
    for d in range(NZ - 1):
        total = total + strecv[d]
    scale = lax.rsqrt(total * (1.0 / (NX * NZ * 128)) + epsilon)
    first_row = (lax.broadcasted_iota(jnp.int32, (8, 128), 0) == 0).astype(f32)
    scol[...] = contract(scale, first_row, ((0,), (0,)), HIGHEST).reshape(NZ, 32, 128)
    r1 = relay(1, d1)
    own_w[3].wait()
    d3 = direct(3)
    absend[...] = jnp.zeros((NZ, 8, 128), f32)
    for r in range(NZ):
        zz = dest(r)
        small = jnp.zeros((16, 32), f32)
        for d in range(NX):
            feature = lax.rem(x + NX - d, NX)
            normed = (xtok[d, zz].astype(f32) * scol[zz] * gainrow[d]).astype(bf16)
            nbuf[r * 32 : (r + 1) * 32, head(d)] = normed
            small = small + contract(abw[:, pl.ds(pl.multiple_of(feature * 128, 128), 128)], normed, ((1,), (1,)))
        absend[r, :, 0:32] = small[0:8]
    ab = [
        go(remote(absend.at[r], abrecv.at[r - 1], abs_.at[r - 1], abr.at[r - 1], at_z(dest(r))))
        for r in range(1, NZ)
    ]

    def project(m, copies):
        arrive(f"far{m}", *copies)
        rows = jnp.dot(nbuf[...], wbuf[m].reshape(512, 512), preferred_element_type=f32)
        if m % 2 == 0:
            yown[m] = rows[0:128]
            y1send[m] = rows[128:256].astype(bf16)
            other = z - side
        else:
            yown[m, 0:32] = rows[0:32]
            yown[m, 32:128] = rows[128:224]
            y1send[m, 0:96] = rows[32:128].astype(bf16)
            y1send[m, 96:128] = rows[224:256].astype(bf16)
            other = z + side
        return go(remote(y1send.at[m], y1recv.at[m], y1s.at[m], y1r.at[m], at_z(other)))

    def second_sum(m, copy):
        arrive(f"pair{m}", copy)
        rows = yown[m] + y1recv[m].astype(f32)
        yown[m, 0:32] = rows[0:32]
        y2send[m] = rows[32:128].astype(bf16).reshape(3, 32, 512)
        way = side if m % 2 == 0 else -side
        return [
            go(remote(y2send.at[m, i - 1], y2recv.at[m, i - 1], y2s.at[m, i - 1], y2r.at[m, i - 1], at_z(z + way * i)))
            for i in (3, 2, 1)
        ]

    def summed(m, copies, lanes):
        rows = yown[m, 0:32, lanes]
        for i in range(3):
            rows = rows + y2recv[m, i, :, lanes].astype(f32)
        return rows

    y1_0 = project(0, r0)
    r2 = relay(2, d2)
    y1_1 = project(1, r1)
    y2_0 = second_sum(0, y1_0)
    r3 = relay(3, d3)
    wos_ = [
        go(remote(wout, wobuf.at[:, pl.ds(d * 128, 128)], wos.at[d - 1], wor.at[d - 1], at_x(x + d)))
        for d in range(1, NX)
    ]
    update_state(4, NB)
    y1_2 = project(2, r2)
    y2_1 = second_sum(1, y1_1)

    arrive("small", *ab)
    small = absend[0]
    for r in range(NZ - 1):
        small = small + abrecv[r]
    soft = jnp.maximum(small, 0.0) + jnp.log1p(jnp.exp(-jnp.abs(small)))
    which = lax.broadcasted_iota(jnp.int32, (8, 128), 0)
    lane = lax.broadcasted_iota(jnp.int32, (8, 32), 1)
    chosen = lane == tp * NH + lax.broadcasted_iota(jnp.int32, (8, 32), 0)
    rates = jnp.sum(jnp.where(chosen, rate[...], 0.0), axis=1, keepdims=True)
    small = jnp.where(which < NH, -rates * soft, 1.0 / (1.0 + jnp.exp(-small)))
    row = lax.broadcasted_iota(jnp.int32, (8, 512), 0)
    lane = lax.broadcasted_iota(jnp.int32, (8, 512), 1) // 128
    logs = contract(small, (row == lane).astype(f32), ((0,), (0,)), HIGHEST)
    strengths = contract(small, (row == lane + NH).astype(f32), ((0,), (0,)), HIGHEST)
    for h in range(NH):
        gnew[h] = logs[0:32, head(h)]
        bnew[h] = strengths[0:32, head(h)]

    y1_3 = project(3, r3)

    def rows_of(ref, t, h):
        return ref[h, pl.ds(t, 8, stride=4)]

    def unit_rows(m, copies, factor):
        arrive(f"sum{m}", *copies)
        for h in range(NH):
            v = silu(summed(m, copies, head(h)))
            tmp[h] = v * lax.rsqrt(across(v * v) + epsilon) * factor
            for t in range(NT):
                kq[h, pl.ds(m * 4 + t, 8, stride=8)] = rows_of(tmp, t, h)

    unit_rows(0, y2_0, 1.0)
    y2_2 = second_sum(2, y1_2)
    unit_rows(1, y2_1, 128**-0.5)
    all_products(kq, 0, 4)
    y2_3 = second_sum(3, y1_3)
    all_products(kq, 4, NB)
    arrive("sum2", *y2_2)
    for h in range(NH):
        vnew[h] = silu(summed(2, y2_2, head(h)))
    for h in range(NH):
        keys = [every(kq, t, h) for t in range(NT)]
        written, decay = delta_rule(
            keys,
            [every(pbuf, t, h) for t in range(NT)],
            [rows_of(vnew, t, h) for t in range(NT)],
            [rows_of(gnew, t, h) for t in range(NT)],
            [rows_of(bnew, t, h) for t in range(NT)],
        )
        for t in range(NT):
            query = every(kq, 4 + t, h)
            attended = decay[t, -1] * every(pbuf, 4 + t, h) + across(keys[t] * query) * written[t]
            for i in range(t):
                attended = attended + decay[t, i] * across(keys[i] * query) * written[i]
            scaled = attended * lax.rsqrt(across(attended * attended) * (1.0 / 128) + epsilon)
            hout[h, pl.ds(t, 8, stride=4)] = scaled * hgain[...]

    arrive("sum3", *y2_3)
    for h in range(NH):
        hsend[:, head(h)] = (hout[h] * silu(summed(3, y2_3, head(h)))).astype(bf16)
    heads = [go(remote(hsend, hz.at[d], hs.at[d - 1], hr.at[d - 1], at_z(z + d))) for d in (4, 3, 5, 2, 6, 1, 7)]
    hz[0] = hsend[...]

    own_wo.wait()
    arrive("wout", *wos_)
    arrive("heads", *heads)
    terms = jnp.dot(hz[...].reshape(256, 512), wobuf[...], preferred_element_type=f32)
    for d in range(NZ):
        zz = lax.rem(z + NZ - d, NZ)
        p3[lax.rem(zz, 2) * NY + zz // 2] = terms[d * 32 : (d + 1) * 32]
    other = go(remote(p3.at[pl.ds((1 - c) * NY, NY)], d2d, tws.at[3], twr.at[3], twin))
    arrive("twin", other)
    for j in range(NY):
        rows = p3[c * NY + j] + d2d[j]
        for e in range(NX):
            psend[j, e] = rows[:, head(e)].astype(bf16)
    parts = [
        go(
            remote(
                psend.at[lax.rem(y + ey, NY), ex], precv.at[ey, ex], ps.at[ey, ex], pr.at[ey, ex],
                {"kv": z * NX + lax.rem(x + NX - ex, NX), "tp": lax.rem(y + ey, NY) * 2 + c},
            )
        )
        for ey, ex in ((2, 2), (2, 1), (2, 3), (1, 2), (3, 2), (2, 0), (0, 2), (1, 1), (1, 3), (3, 1), (3, 3), (1, 0), (3, 0), (0, 1), (0, 3))
    ]
    own_part = p3[c * NY + y, :, 0:128] + d2d[y, :, 0:128]
    arrive("parts", *parts)
    for ex in range(NX):
        total = own_part if ex == 0 else precv[0, ex].astype(f32)
        for ey in range(1, NY):
            total = total + precv[ey, ex].astype(f32)
        mixed[lax.rem(x + ex, NX)] = total.astype(bf16)
    with jax.named_scope("drain"):
        for copy in pending:
            copy.wait_send()


def fused(*operands):
    anywhere = pl.BlockSpec(memory_space=pl.ANY)
    vmem = pl.BlockSpec(memory_space=pltpu.VMEM)
    dma = pltpu.SemaphoreType.DMA
    scratch = [
        pltpu.VMEM((NX * NZ, 128), f32),
        pltpu.VMEM((32, 512), bf16),
        pltpu.VMEM((32, 512), bf16),
        pltpu.VMEM((128, 128), bf16),
        pltpu.VMEM((128, 128), bf16),
        pltpu.VMEM((16, 8), f32),
        pltpu.VMEM((16, 8), f32),
        pltpu.VMEM((1, 8), jnp.int32),
        pltpu.VMEM((1, 32), f32),
        pltpu.VMEM((1, 128), f32),
        dma((10,)),
        pltpu.VMEM((128, 128), f32),
        pltpu.VMEM((128, 128), f32),
        pltpu.VMEM((NH, 64, 128), f32),
        pltpu.VMEM((8, 2048), f32),
        pltpu.VMEM((8, 2048), f32),
        pltpu.VMEM((16, 512), bf16),
        pltpu.VMEM((NX, 1, 128), f32),
        pltpu.VMEM((NZ, NX, 32, 128), bf16),
        pltpu.VMEM((NX, NZ, 32, 128), bf16),
        pltpu.VMEM((4, NX, 128, 512), bf16),
        pltpu.VMEM((8, 256), f32),
        pltpu.VMEM((NZ - 1, 8, 256), f32),
        pltpu.VMEM((NZ, 32, 128), f32),
        pltpu.VMEM((256, 512), bf16),
        pltpu.VMEM((NZ, 8, 128), f32),
        pltpu.VMEM((NZ - 1, 8, 128), f32),
        pltpu.VMEM((4, 128, 512), f32),
        pltpu.VMEM((4, 128, 512), bf16),
        pltpu.VMEM((4, 128, 512), bf16),
        pltpu.VMEM((4, 3, 32, 512), bf16),
        pltpu.VMEM((4, 3, 32, 512), bf16),
        pltpu.VMEM((512, 512), bf16),
        pltpu.VMEM((NH, 64, 128), f32),
        pltpu.VMEM((NH, 64, 128), f32),
        pltpu.VMEM((NH, 64, 128), f32),
        pltpu.VMEM((NH, 32, 128), f32),
        pltpu.VMEM((NH, 64, 128), f32),
        pltpu.VMEM((NH, 32, 128), f32),
        pltpu.VMEM((NH, 32, 128), f32),
        pltpu.VMEM((NH, 32, 128), f32),
        pltpu.VMEM((NH, 32, 128), f32),
        pltpu.VMEM((32, 512), bf16),
        pltpu.VMEM((NZ, 32, 512), bf16),
        pltpu.VMEM((NZ, 32, 512), f32),
        pltpu.VMEM((NY, 32, 512), f32),
        pltpu.VMEM((NY, NX, 32, 128), bf16),
        pltpu.VMEM((NY, NX, 32, 128), bf16),
        dma((8,)),
        dma((3,)), dma((3,)),
        dma((4, 2)), dma((4, 2)), dma((4, 2)), dma((4, 2)),
        dma((7,)), dma((7,)), dma((7,)), dma((7,)),
        dma((4,)), dma((4,)), dma((4, 3)), dma((4, 3)),
        dma((3,)), dma((3,)),
        dma((7,)), dma((7,)),
        dma((4,)), dma((4,)),
        dma((NY, NX)), dma((NY, NX)),
    ]
    return pl.pallas_call(
        kernel,
        out_shape=(
            pltpu.VMEM((NX, 32, 128), bf16),
            pltpu.VMEM((NB * NH, 128, 128), f32),
        ),
        in_specs=[anywhere] * 17,
        out_specs=(vmem, vmem),
        scratch_shapes=scratch,
        compiler_params=pltpu.CompilerParams(collective_id=0, has_side_effects=True),
        name="step",
    )(*operands)


def per_device(
    tokens,
    norm_gain,
    w_query,
    w_key,
    w_value,
    w_gate,
    w_decay,
    w_beta,
    decay_rate,
    head_gain,
    w_out,
    state,
    prev_keys,
    prev_values,
    prev_log_decay,
    prev_beta,
    accepted,
):
    mixed, carried = fused(
        tokens.reshape(NZ, NX, 32, 128), w_key, w_query, w_value, w_gate, w_out,
        state.reshape(NB * NH, 128, 128), norm_gain.reshape(NX * NZ, 128), w_decay.T, w_beta.T,
        prev_keys.reshape(128, 128), prev_values.reshape(128, 128),
        prev_log_decay.transpose(1, 2, 0).reshape(16, NB), prev_beta.transpose(1, 2, 0).reshape(16, NB),
        accepted.reshape(1, NB), decay_rate.reshape(1, 32), head_gain.reshape(1, 128),
    )
    return mixed.reshape(32, NT, 128), carried.reshape(NB, NH, 128, 128)


def solution(mesh):
    placed = (
        P(None, None, "kv"),
        P(),
        P("kv", "tp"),
        P("kv", "tp"),
        P("kv", "tp"),
        P("kv", "tp"),
        P(),
        P(),
        P(),
        P(),
        P("tp", "kv"),
        P("kv", "tp", None, None),
        P("kv", "tp", None, None),
        P("kv", "tp", None, None),
        P("kv", "tp", None),
        P("kv", "tp", None),
        P("kv"),
    )
    return jax.shard_map(
        per_device,
        mesh=mesh,
        in_specs=placed,
        out_specs=(P("tp", None, "kv"), P("kv", "tp", None, None)),
        check_vma=False,
    )
```

```python
import jax
import jax.numpy as jnp
from jax import lax
from jax.experimental import pallas as pl
from jax.experimental.pallas import tpu as pltpu
from jax.sharding import PartitionSpec as P

MESH = pl.DeviceIdType.MESH
HIGHEST = lax.Precision.HIGHEST
epsilon = 1e-06

NZ, NX, NY, NT, NB, NH = 8, 4, 4, 4, 8, 4
f32, bf16 = jnp.float32, jnp.bfloat16
NC, WIDE = 8, 256
CHUNKS = tuple(slice(i * WIDE, (i + 1) * WIDE) for i in range(NC))


def contract(a, b, dims, precision=None):
    return lax.dot_general(a, b, (dims, ((), ())), precision=precision, preferred_element_type=f32)


def silu(v):
    return v / (1.0 + jnp.exp(-v))


def head(h):
    return slice(h * 128, (h + 1) * 128)


def across(v):
    return jnp.sum(v, axis=-1, keepdims=True)


def delta_rule(keys, predicted, values, logs, betas):
    decay = {}
    for t in range(NT):
        total = logs[t]
        decay[t, t] = None
        for i in range(t - 1, -1, -1):
            decay[t, i] = jnp.exp(total)
            total = total + logs[i]
        decay[t, -1] = jnp.exp(total)
    written = []
    for t in range(NT):
        expected = decay[t, -1] * predicted[t]
        for i in range(t):
            expected = expected + decay[t, i] * across(keys[i] * keys[t]) * written[i]
        written.append(betas[t] * (values[t] - expected))
    return written, decay


def kernel(
    tok, wkey, wquery, wvalue, wgate, wout, state, *rest
):
    small_in, (mixed, sbuf, *rest) = rest[:10], rest[10:]
    small_ref, rest = rest[:10], rest[10:]
    gain, wdecay, wbeta, pkeys, pvalues, plogs, pbetas, accepted, rate, hgain = small_ref
    (
    small_sem, kraw, vraw, kold, gold, bold, abw, gainrow, tokbuf, xtok, wbuf, sqsend, sqrecv, stsend, strecv, scol, nbuf, absend, abrecv,
    yown, y1send, y1recv, y2send, y2recv, wobuf, halves, pbuf, ubuf, ebuf, tmp, kq, gnew, bnew, vnew, hout,
    hsend, hz, p3, d2d, psend, precv,
    loc, tr, wdr, wrr, y1r, y2r, hr, hs, sent, got, wave,
    ) = rest
    s_sq, s_tok, s_direct, s_relay, s_stat, s_small, s_y1, s_y2, s_wo, s_twin, s_d2d, s_part = [sent.at[i] for i in range(12)]
    r_sq, r_stat, r_small, r_wo, r_twin, r_d2d, r_part = [got.at[i] for i in range(7)]
    kv, tp = lax.axis_index("kv"), lax.axis_index("tp")
    z, x, y, c = kv // NX, lax.rem(kv, NX), tp // 2, lax.rem(tp, 2)
    side = 2 * lax.rem(z, 2) - 1
    weights = (wkey, wquery, wvalue, wgate)

    def at_z(zz):
        return {"kv": lax.rem(zz + 2 * NZ, NZ) * NX + x}

    def at_x(xx):
        return {"kv": z * NX + lax.rem(xx + NX, NX)}

    def dest(r):
        off = side * r if r < 4 else -side * (r - 3)
        return lax.rem(z + off + 2 * NZ, NZ)

    def remote(src, dst, send, recv, device):
        return pltpu.make_async_remote_copy(
            src_ref=src, dst_ref=dst, send_sem=send, recv_sem=recv, device_id=device, device_id_type=MESH
        )

    twin = {"tp": tp + 1 - 2 * c}

    def go(copy):
        copy.start()
        return copy

    def arrive(name, ref, sem):
        with jax.named_scope(name):
            pltpu.make_async_copy(ref, ref, sem).wait()

    barrier = pltpu.get_barrier_semaphore()
    near = [at_x(x + d) for d in (1, 3, 2)] + [at_z(z + 1), at_z(z - 1)]
    near += [{"tp": lax.rem(y + d, NY) * 2 + c} for d in (1, 3, 2)]
    for there in near:
        pl.semaphore_signal(barrier, inc=1, device_id=there, device_id_type=MESH)
    pl.semaphore_signal(barrier, inc=1, device_id=twin, device_id_type=MESH)

    own_tok = pltpu.make_async_copy(tok, tokbuf, loc.at[0])
    own_tok.start()
    own_w = []
    for i, lanes in enumerate(CHUNKS):
        m, start = lanes.start // 512, lanes.start % 512
        part = weights[m].at[:, pl.ds(start, lanes.stop - lanes.start)]
        own_w.append(pltpu.make_async_copy(part, wbuf.at[0, :, lanes], loc.at[3 + i]))
    for copy in own_w:
        copy.start()
    sources = list(small_in)
    for i in (1, 2):
        sources[i] = small_in[i].at[:, pl.ds(pl.multiple_of(z * 512, 512), 512)]
    own_small = [pltpu.make_async_copy(a, b, small_sem.at[i]) for i, (a, b) in enumerate(zip(sources, small_ref))]
    for copy in own_small:
        copy.start()
    own_s = pltpu.make_async_copy(state, sbuf, loc.at[1])
    own_s.start()
    own_wo = pltpu.make_async_copy(wout, wobuf.at[:, 0:128], loc.at[2])
    own_wo.start()

    own_tok.wait()
    for e in range(NX):
        squares = tokbuf[:, e].reshape(NZ * 32, 128).astype(f32)
        sqsend[e] = contract(jnp.ones((8, 128), f32), squares * squares, ((1,), (1,)), HIGHEST)[0:1]
    for copy in own_w:
        copy.wait()
    with jax.named_scope("barrier"):
        pl.semaphore_wait(barrier, len(near) + 1)

    for d in (2, 1, 3):
        go(remote(sqsend.at[lax.rem(x + d, NX)], sqrecv.at[d - 1], s_sq, r_sq, at_x(x + d)))

    mine, theirs = pl.ds(c * 4, 4), pl.ds(4 - c * 4, 4)
    for d in (2, 1, 3):
        go(remote(tokbuf.at[mine, lax.rem(x + d, NX)], xtok.at[d, mine], s_tok, tr.at[d - 1], at_x(x + d)))

    low, high = slice(0, 64), slice(64, 128)

    def direct(i):
        lanes = CHUNKS[i]
        go(remote(wbuf.at[0, :, lanes], wbuf.at[1, :, lanes], s_direct, wdr.at[i, 0], at_x(x + 1)))
        go(remote(wbuf.at[0, :, lanes], wbuf.at[3, :, lanes], s_direct, wdr.at[i, 1], at_x(x + 3)))

    def relay(i):
        lanes = CHUNKS[i]
        arrive(f"left{i}", wbuf.at[1, :, lanes], wdr.at[i, 0])
        go(remote(wbuf.at[1, low, lanes], wbuf.at[2, low, lanes], s_relay, wrr.at[i], at_x(x + 1)))
        arrive(f"right{i}", wbuf.at[3, :, lanes], wdr.at[i, 1])
        go(remote(wbuf.at[3, high, lanes], wbuf.at[2, high, lanes], s_relay, wrr.at[i], at_x(x + 3)))

    direct(0)
    direct(1)
    direct(2)

    def products(left, b, h):
        rows = pl.ds(pl.multiple_of(b * 8, 8), 8)
        pbuf[h, rows] = contract(left[h, rows], sbuf[b * NH + h], ((1,), (0,)), HIGHEST)

    def all_products(left, first, last):
        @pl.loop(first, last)
        def _(b):
            for h in range(NH):
                products(left, b, h)

    def every(ref, start, h):
        return ref[h, pl.ds(start, 8, stride=8)]

    def update_state(first, last):
        @pl.loop(first, last)
        def _(b):
            rows = pl.ds(pl.multiple_of(b * 8, 8), 8)
            for h in range(NH):
                added = contract(kold[h, rows], ubuf[h, rows], ((0,), (0,)), HIGHEST)
                matrix = sbuf[b * NH + h] * ebuf[h, rows][0:1] + added
                sbuf[b * NH + h] = matrix
                large = matrix.astype(bf16)
                halves[b * NH + h, 0:128] = large
                halves[b * NH + h, 128:256] = (matrix - large.astype(f32)).astype(bf16)

    def spread(k):
        pl.semaphore_signal(wave.at[k], inc=1, device_id=at_z(z + 1), device_id_type=MESH)
        pl.semaphore_signal(wave.at[k], inc=1, device_id=at_z(z - 1), device_id_type=MESH)

    spread(0)

    for copy in own_small:
        copy.wait()
    row = lax.broadcasted_iota(jnp.int32, (16, 32), 0)
    col = lax.broadcasted_iota(jnp.int32, (16, 32), 1) - tp * NH
    abw[...] = (
        contract(((row == col) & (row < NH)).astype(bf16), wdecay[...], ((1,), (0,)))
        + contract(((row == col + NH) & (row >= NH) & (row < 2 * NH)).astype(bf16), wbeta[...], ((1,), (0,)))
    ).astype(bf16)
    row = lax.broadcasted_iota(jnp.int32, (NX * NZ, 128), 0)
    for d in range(NX):
        here = row == z * NX + lax.rem(x + NX - d, NX)
        gainrow[d] = jnp.sum(jnp.where(here, gain[...], 0.0), axis=0, keepdims=True)
    pl.semaphore_wait(wave.at[0], 2)
    spread(1)
    keys = pkeys[...].astype(f32)
    kraw[...] = keys * lax.rsqrt(across(keys * keys) + epsilon)
    vraw[...] = pvalues[...].astype(f32)
    for h in range(NH):
        for t in range(NT):
            kold[h, pl.ds(t, 8, stride=8)] = kraw[pl.ds(h * NT + t, 8, stride=16)]
            kold[h, pl.ds(t + 4, 8, stride=8)] = jnp.zeros((8, 128), f32)
    kept = lax.rem(lax.broadcasted_iota(jnp.int32, (16, 8), 0), NT) < accepted[...]
    apart = lax.broadcasted_iota(jnp.int32, (16, 2048), 0) == lax.broadcasted_iota(jnp.int32, (16, 2048), 1) // 128
    apart = apart.astype(f32)
    gold[...] = contract(jnp.where(kept, plogs[...], 0.0), apart, ((0,), (0,)), HIGHEST)
    bold[...] = contract(jnp.where(kept, pbetas[...], 0.0), apart, ((0,), (0,)), HIGHEST)
    pl.semaphore_wait(wave.at[1], 2)
    spread(2)
    own_s.wait()
    all_products(kold, 0, 2)
    arrive("squares", sqrecv, r_sq)
    with jax.named_scope("wave"):
        pl.semaphore_wait(wave.at[2], 2)
    stsend[...] = ((sqsend[x] + sqrecv[0]) + sqrecv[1]) + sqrecv[2]
    for d in (4, 3, 5, 2, 6, 1, 7):
        go(remote(stsend, strecv.at[d - 1], s_stat, r_stat, at_z(z + d)))
    for d in (1, 3, 2):
        arrive(f"tokens{d}", xtok.at[d, mine], tr.at[d - 1])
        go(remote(xtok.at[d, mine], xtok.at[d, mine], s_twin, r_twin, twin))
    xtok[0] = tokbuf[:, x]
    relay(0)
    direct(3)
    all_products(kold, 2, NB)
    relay(1)
    direct(4)
    arrive("tokens", xtok.at[1:4, theirs], r_twin)

    for h in range(NH):
        keys = [every(kold, t, h) for t in range(NT)]
        written, decay = delta_rule(
            keys,
            [every(pbuf, t, h) for t in range(NT)],
            [vraw[pl.ds(h * NT + t, 8, stride=16)] for t in range(NT)],
            [gold[:, head(h * NT + t)] for t in range(NT)],
            [bold[:, head(h * NT + t)] for t in range(NT)],
        )
        for t in range(NT):
            last = written[t] if t == NT - 1 else decay[NT - 1, t] * written[t]
            ubuf[h, pl.ds(t, 8, stride=8)] = last
            ubuf[h, pl.ds(t + 4, 8, stride=8)] = jnp.zeros((8, 128), f32)
        ebuf[h, pl.ds(0, 8, stride=8)] = decay[NT - 1, -1]
    relay(2)
    direct(5)

    arrive("stats", strecv, r_stat)
    total = stsend[...]
    for d in range(NZ - 1):
        total = total + strecv[d]
    scale = lax.rsqrt(total * (1.0 / (NX * NZ * 128)) + epsilon)
    first_row = (lax.broadcasted_iota(jnp.int32, (8, 128), 0) == 0).astype(f32)
    scol[...] = contract(jnp.broadcast_to(scale, (8, 256)), first_row, ((0,), (0,)), HIGHEST).reshape(NZ, 32, 128)
    absend[...] = jnp.zeros((NZ, 8, 128), f32)
    for r in range(NZ):
        zz = dest(r)
        small = jnp.zeros((16, 32), f32)
        for d in range(NX):
            feature = lax.rem(x + NX - d, NX)
            normed = (xtok[d, zz].astype(f32) * scol[zz] * gainrow[d]).astype(bf16)
            nbuf[r * 32 : (r + 1) * 32, head(d)] = normed
            small = small + contract(abw[:, pl.ds(pl.multiple_of(feature * 128, 128), 128)], normed, ((1,), (1,)))
        absend[r, :, 0:32] = small[0:8]
    for r in range(1, NZ):
        go(remote(absend.at[r], abrecv.at[r - 1], s_small, r_small, at_z(dest(r))))
    def project(i):
        lanes = CHUNKS[i]
        arrive(f"far{i}", wbuf.at[2, :, lanes], wrr.at[i])
        rows = jnp.dot(
            nbuf[...], wbuf[:, :, lanes].reshape(512, lanes.stop - lanes.start), preferred_element_type=f32
        )
        if i % 2 == 0:
            yown[:, lanes] = rows[0:128]
            y1send[:, lanes] = rows[128:256].astype(bf16)
            other = z - side
        else:
            yown[0:32, lanes] = rows[0:32]
            yown[32:128, lanes] = rows[128:224]
            y1send[0:96, lanes] = rows[32:128].astype(bf16)
            y1send[96:128, lanes] = rows[224:256].astype(bf16)
            other = z + side
        go(remote(y1send.at[:, lanes], y1recv.at[:, lanes], s_y1, y1r.at[i], at_z(other)))

    def second_sum(i):
        lanes = CHUNKS[i]
        arrive(f"pair{i}", y1recv.at[:, lanes], y1r.at[i])
        rows = yown[:, lanes] + y1recv[:, lanes].astype(f32)
        yown[0:32, lanes] = rows[0:32]
        for j in range(3):
            y2send[j, :, lanes] = rows[32 * (j + 1) : 32 * (j + 2)].astype(bf16)
        way = side if i % 2 == 0 else -side
        for j in (3, 2, 1):
            go(remote(y2send.at[j - 1, :, lanes], y2recv.at[j - 1, :, lanes], s_y2, y2r.at[i], at_z(z + way * j)))

    def last_sum(i):
        lanes = CHUNKS[i]
        arrive(f"sum{i}", y2recv.at[:, :, lanes], y2r.at[i])

    def summed(m, h):
        lanes = head(m * NH + h)
        rows = yown[0:32, lanes]
        for j in range(3):
            rows = rows + y2recv[j, :, lanes].astype(f32)
        return rows

    project(0)
    relay(3)
    direct(6)
    project(1)
    update_state(0, 2)
    relay(4)
    direct(7)
    project(2)
    relay(5)
    update_state(2, 3)
    project(3)
    second_sum(0)
    relay(6)
    update_state(3, 4)
    second_sum(1)
    project(4)
    relay(7)
    own_wo.wait()
    for d in range(1, NX):
        go(remote(wobuf.at[:, 0:128], wobuf.at[:, d * 128 : (d + 1) * 128], s_wo, r_wo, at_x(x + d)))
    update_state(4, 5)
    second_sum(2)
    project(5)
    project(6)
    second_sum(3)
    project(7)
    update_state(5, NB)
    second_sum(4)

    arrive("small", abrecv, r_small)
    small = absend[0]
    for r in range(NZ - 1):
        small = small + abrecv[r]
    soft = jnp.maximum(small, 0.0) + jnp.log1p(jnp.exp(-jnp.abs(small)))
    which = lax.broadcasted_iota(jnp.int32, (8, 128), 0)
    lane = lax.broadcasted_iota(jnp.int32, (8, 32), 1)
    chosen = lane == tp * NH + lax.broadcasted_iota(jnp.int32, (8, 32), 0)
    rates = jnp.sum(jnp.where(chosen, rate[...], 0.0), axis=1, keepdims=True)
    small = jnp.where(which < NH, -rates * soft, 1.0 / (1.0 + jnp.exp(-small)))
    row = lax.broadcasted_iota(jnp.int32, (8, 512), 0)
    lane = lax.broadcasted_iota(jnp.int32, (8, 512), 1) // 128
    logs = contract(small, (row == lane).astype(f32), ((0,), (0,)), HIGHEST)
    strengths = contract(small, (row == lane + NH).astype(f32), ((0,), (0,)), HIGHEST)
    for h in range(NH):
        gnew[h] = logs[0:32, head(h)]
        bnew[h] = strengths[0:32, head(h)]

    def rows_of(ref, t, h):
        return ref[h, pl.ds(t, 8, stride=4)]

    def unit_rows(m, factor):
        for h in range(NH):
            v = silu(summed(m, h))
            tmp[h] = v * lax.rsqrt(across(v * v) + epsilon) * factor
            for t in range(NT):
                kq[h, pl.ds(m * 4 + t, 8, stride=8)] = rows_of(tmp, t, h)

    second_sum(5)
    second_sum(6)
    last_sum(0)
    last_sum(1)
    unit_rows(0, 1.0)
    second_sum(7)
    last_sum(2)
    last_sum(3)
    unit_rows(1, 128**-0.5)

    @pl.loop(0, NB)
    def _(b):
        rows = pl.ds(pl.multiple_of(b * 8, 8), 8)
        for h in range(NH):
            left = kq[h, rows]
            large = left.astype(bf16).astype(f32)
            left = jnp.concatenate(
                [jnp.concatenate([large, large], axis=1), jnp.concatenate([left - large, jnp.zeros_like(left)], axis=1)],
                axis=0,
            )
            both = contract(left.astype(bf16), halves[b * NH + h], ((1,), (0,)))
            pbuf[h, rows] = both[0:8] + both[8:16]

    last_sum(4)
    last_sum(5)
    for h in range(NH):
        vnew[h] = silu(summed(2, h))
    for h in range(NH):
        keys = [every(kq, t, h) for t in range(NT)]
        written, decay = delta_rule(
            keys,
            [every(pbuf, t, h) for t in range(NT)],
            [rows_of(vnew, t, h) for t in range(NT)],
            [rows_of(gnew, t, h) for t in range(NT)],
            [rows_of(bnew, t, h) for t in range(NT)],
        )
        for t in range(NT):
            query = every(kq, 4 + t, h)
            attended = decay[t, -1] * every(pbuf, 4 + t, h) + across(keys[t] * query) * written[t]
            for i in range(t):
                attended = attended + decay[t, i] * across(keys[i] * query) * written[i]
            scaled = attended * lax.rsqrt(across(attended * attended) * (1.0 / 128) + epsilon)
            hout[h, pl.ds(t, 8, stride=4)] = scaled * hgain[...]

    for g in range(2):
        last_sum(6 + g)
        for h in (2 * g, 2 * g + 1):
            hsend[g, :, head(h - 2 * g)] = (hout[h] * silu(summed(3, h))).astype(bf16)
        for d in (4, 3, 5, 2, 6, 1, 7):
            go(remote(hsend.at[g], hz.at[g, d], hs.at[g], hr.at[g], at_z(z + d)))
        hz[g, 0] = hsend[g]

    arrive("wout", wobuf.at[:, 128:512], r_wo)
    arrive("heads0", hz.at[0, 1:8], hr.at[0])
    terms = jnp.dot(hz[0].reshape(256, 256), wobuf[0:256], preferred_element_type=f32)
    arrive("heads1", hz.at[1, 1:8], hr.at[1])
    terms = terms + jnp.dot(hz[1].reshape(256, 256), wobuf[256:512], preferred_element_type=f32)
    for d in range(NZ):
        zz = lax.rem(z + NZ - d, NZ)
        p3[lax.rem(zz, 2) * NY + zz // 2] = terms[d * 32 : (d + 1) * 32]
    go(remote(p3.at[pl.ds((1 - c) * NY, NY)], d2d, s_d2d, r_d2d, twin))
    arrive("twin", d2d, r_d2d)
    for j in range(NY):
        rows = p3[c * NY + j] + d2d[j]
        for e in range(NX):
            psend[j * NX + e] = rows[:, head(e)].astype(bf16)
    for ey, ex in (
        (2, 2), (2, 1), (2, 3), (1, 2), (3, 2), (2, 0), (0, 2), (1, 1), (1, 3), (3, 1), (3, 3), (1, 0), (3, 0), (0, 1), (0, 3),
    ):
        there = {"kv": z * NX + lax.rem(x + NX - ex, NX), "tp": lax.rem(y + ey, NY) * 2 + c}
        go(remote(psend.at[lax.rem(y + ey, NY) * NX + ex], precv.at[ey * NX + ex], s_part, r_part, there))
    own_part = p3[c * NY + y, :, 0:128] + d2d[y, :, 0:128]
    arrive("parts", precv.at[1:16], r_part)
    for ex in range(NX):
        total = own_part if ex == 0 else precv[ex].astype(f32)
        for ey in range(1, NY):
            total = total + precv[ey * NX + ex].astype(f32)
        mixed[lax.rem(x + ex, NX)] = total.astype(bf16)
    for ref, sem in (
        (xtok.at[1:4, mine], s_tok), (wbuf.at[0:2], s_direct), (wbuf.at[0], s_relay), (sqrecv, s_sq), (strecv, s_stat), (abrecv, s_small),
        (y1send, s_y1), (y2send, s_y2), (wobuf.at[:, 128:512], s_wo), (xtok.at[1:4, mine], s_twin), (d2d, s_d2d),
        (hz.at[0, 1:8], hs.at[0]), (hz.at[1, 1:8], hs.at[1]), (precv.at[1:16], s_part),
    ):
        arrive("drain", ref, sem)


def fused(*operands):
    anywhere = pl.BlockSpec(memory_space=pl.ANY)
    vmem = pl.BlockSpec(memory_space=pltpu.VMEM)
    dma = pltpu.SemaphoreType.DMA
    scratch = [
        pltpu.VMEM((NX * NZ, 128), f32),
        pltpu.VMEM((32, 512), bf16),
        pltpu.VMEM((32, 512), bf16),
        pltpu.VMEM((128, 128), bf16),
        pltpu.VMEM((128, 128), bf16),
        pltpu.VMEM((16, 8), f32),
        pltpu.VMEM((16, 8), f32),
        pltpu.VMEM((1, 8), jnp.int32),
        pltpu.VMEM((1, 32), f32),
        pltpu.VMEM((1, 128), f32),
        dma((10,)),
        pltpu.VMEM((128, 128), f32),
        pltpu.VMEM((128, 128), f32),
        pltpu.VMEM((NH, 64, 128), f32),
        pltpu.VMEM((8, 2048), f32),
        pltpu.VMEM((8, 2048), f32),
        pltpu.VMEM((16, 512), bf16),
        pltpu.VMEM((NX, 1, 128), f32),
        pltpu.VMEM((NZ, NX, 32, 128), bf16),
        pltpu.VMEM((NX, NZ, 32, 128), bf16),
        pltpu.VMEM((NX, 128, 2048), bf16),
        pltpu.VMEM((NX, 1, 256), f32),
        pltpu.VMEM((NX - 1, 1, 256), f32),
        pltpu.VMEM((1, 256), f32),
        pltpu.VMEM((NZ - 1, 1, 256), f32),
        pltpu.VMEM((NZ, 32, 128), f32),
        pltpu.VMEM((256, 512), bf16),
        pltpu.VMEM((NZ, 8, 128), f32),
        pltpu.VMEM((NZ - 1, 8, 128), f32),
        pltpu.VMEM((128, 2048), f32),
        pltpu.VMEM((128, 2048), bf16),
        pltpu.VMEM((128, 2048), bf16),
        pltpu.VMEM((3, 32, 2048), bf16),
        pltpu.VMEM((3, 32, 2048), bf16),
        pltpu.VMEM((512, 512), bf16),
        pltpu.VMEM((NB * NH, 256, 128), bf16),
        pltpu.VMEM((NH, 64, 128), f32),
        pltpu.VMEM((NH, 64, 128), f32),
        pltpu.VMEM((NH, 64, 128), f32),
        pltpu.VMEM((NH, 32, 128), f32),
        pltpu.VMEM((NH, 64, 128), f32),
        pltpu.VMEM((NH, 32, 128), f32),
        pltpu.VMEM((NH, 32, 128), f32),
        pltpu.VMEM((NH, 32, 128), f32),
        pltpu.VMEM((NH, 32, 128), f32),
        pltpu.VMEM((2, 32, 256), bf16),
        pltpu.VMEM((2, NZ, 32, 256), bf16),
        pltpu.VMEM((NZ, 32, 512), f32),
        pltpu.VMEM((NY, 32, 512), f32),
        pltpu.VMEM((NY * NX, 32, 128), bf16),
        pltpu.VMEM((NY * NX, 32, 128), bf16),
        dma((3 + NC,)),
        dma((3,)),
        dma((NC, 2)),
        dma((NC,)),
        dma((NC,)),
        dma((NC,)),
        dma((2,)),
        dma((2,)),
        dma((12,)),
        dma((7,)),
        pltpu.SemaphoreType.REGULAR((3,)),
    ]
    return pl.pallas_call(
        kernel,
        out_shape=(
            pltpu.VMEM((NX, 32, 128), bf16),
            pltpu.VMEM((NB * NH, 128, 128), f32),
        ),
        in_specs=[anywhere] * 17,
        out_specs=(vmem, vmem),
        scratch_shapes=scratch,
        compiler_params=pltpu.CompilerParams(collective_id=0, has_side_effects=True),
        name="step",
    )(*operands)


def per_device(
    tokens,
    norm_gain,
    w_query,
    w_key,
    w_value,
    w_gate,
    w_decay,
    w_beta,
    decay_rate,
    head_gain,
    w_out,
    state,
    prev_keys,
    prev_values,
    prev_log_decay,
    prev_beta,
    accepted,
):
    mixed, carried = fused(
        tokens.reshape(NZ, NX, 32, 128), w_key, w_query, w_value, w_gate, w_out,
        state.reshape(NB * NH, 128, 128), norm_gain.reshape(NX * NZ, 128), w_decay.T, w_beta.T,
        prev_keys.reshape(128, 128), prev_values.reshape(128, 128),
        prev_log_decay.transpose(1, 2, 0).reshape(16, NB), prev_beta.transpose(1, 2, 0).reshape(16, NB),
        accepted.reshape(1, NB), decay_rate.reshape(1, 32), head_gain.reshape(1, 128),
    )
    return mixed.reshape(32, NT, 128), carried.reshape(NB, NH, 128, 128)


def solution(mesh):
    placed = (
        P(None, None, "kv"),
        P(),
        P("kv", "tp"),
        P("kv", "tp"),
        P("kv", "tp"),
        P("kv", "tp"),
        P(),
        P(),
        P(),
        P(),
        P("tp", "kv"),
        P("kv", "tp", None, None),
        P("kv", "tp", None, None),
        P("kv", "tp", None, None),
        P("kv", "tp", None),
        P("kv", "tp", None),
        P("kv"),
    )
    return jax.shard_map(
        per_device,
        mesh=mesh,
        in_specs=placed,
        out_specs=(P("tp", None, "kv"), P("kv", "tp", None, None)),
        check_vma=False,
    )
```

```python
import jax
import jax.numpy as jnp
from jax import lax
from jax.experimental import pallas as pl
from jax.experimental.pallas import tpu as pltpu
from jax.sharding import PartitionSpec as P

MESH = pl.DeviceIdType.MESH
HIGHEST = lax.Precision.HIGHEST
epsilon = 1e-06

NZ, NX, NY, NT, NB, NH = 8, 4, 4, 4, 8, 4
f32, bf16 = jnp.float32, jnp.bfloat16
NC, WIDE = 8, 256
CHUNKS = tuple(slice(i * WIDE, (i + 1) * WIDE) for i in range(NC))


def contract(a, b, dims, precision=None):
    return lax.dot_general(a, b, (dims, ((), ())), precision=precision, preferred_element_type=f32)


def silu(v):
    return v / (1.0 + jnp.exp(-v))


def head(h):
    return slice(h * 128, (h + 1) * 128)


def across(v):
    return jnp.sum(v, axis=-1, keepdims=True)


def delta_rule(keys, predicted, values, logs, betas):
    decay = {}
    for t in range(NT):
        total = logs[t]
        decay[t, t] = None
        for i in range(t - 1, -1, -1):
            decay[t, i] = jnp.exp(total)
            total = total + logs[i]
        decay[t, -1] = jnp.exp(total)
    written = []
    for t in range(NT):
        expected = decay[t, -1] * predicted[t]
        for i in range(t):
            expected = expected + decay[t, i] * across(keys[i] * keys[t]) * written[i]
        written.append(betas[t] * (values[t] - expected))
    return written, decay


def kernel(
    tok, wkey, wquery, wvalue, wgate, wout, state, *rest
):
    small_in, (mixed, sbuf, *rest) = rest[:10], rest[10:]
    small_ref, rest = rest[:10], rest[10:]
    gain, wdecay, wbeta, pkeys, pvalues, plogs, pbetas, accepted, rate, hgain = small_ref
    (
    small_sem, kraw, vraw, kold, gold, bold, abw, gainrow, tokbuf, xtok, wbuf, sqsend, sqrecv, stsend, strecv, scol, nbuf, absend, abrecv,
    yown, y1send, y1recv, y2send, y2recv, wobuf, halves, pbuf, ubuf, ebuf, tmp, kq, gnew, bnew, vnew, hout,
    hsend, hz, p3, d2d, psend, precv,
    loc, tr, wdr, wrr, y1r, y2r, hr, hs, sent, got, wave,
    ) = rest
    s_sq, s_tok, s_direct, s_relay, s_stat, s_small, s_y1, s_y2, s_wo, s_twin, s_d2d, s_part = [sent.at[i] for i in range(12)]
    r_sq, r_stat, r_small, r_wo, r_twin, r_d2d, r_part = [got.at[i] for i in range(7)]
    kv, tp = lax.axis_index("kv"), lax.axis_index("tp")
    z, x, y, c = kv // NX, lax.rem(kv, NX), tp // 2, lax.rem(tp, 2)
    side = 2 * lax.rem(z, 2) - 1
    weights = (wkey, wquery, wvalue, wgate)

    def at_z(zz):
        return {"kv": lax.rem(zz + 2 * NZ, NZ) * NX + x}

    def at_x(xx):
        return {"kv": z * NX + lax.rem(xx + NX, NX)}

    def dest(r):
        off = side * r if r < 4 else -side * (r - 3)
        return lax.rem(z + off + 2 * NZ, NZ)

    def remote(src, dst, send, recv, device):
        return pltpu.make_async_remote_copy(
            src_ref=src, dst_ref=dst, send_sem=send, recv_sem=recv, device_id=device, device_id_type=MESH
        )

    twin = {"tp": tp + 1 - 2 * c}

    def go(copy):
        copy.start()
        return copy

    def arrive(name, ref, sem):
        with jax.named_scope(name):
            pltpu.make_async_copy(ref, ref, sem).wait()

    barrier = pltpu.get_barrier_semaphore()
    near = [at_x(x + d) for d in (1, 3, 2)] + [at_z(z + 1), at_z(z - 1)]
    near += [{"tp": lax.rem(y + d, NY) * 2 + c} for d in (1, 3, 2)]
    for there in near:
        pl.semaphore_signal(barrier, inc=1, device_id=there, device_id_type=MESH)
    pl.semaphore_signal(barrier, inc=1, device_id=twin, device_id_type=MESH)

    own_tok = pltpu.make_async_copy(tok, tokbuf, loc.at[0])
    own_tok.start()
    own_w = []
    for i, lanes in enumerate(CHUNKS):
        m, start = lanes.start // 512, lanes.start % 512
        part = weights[m].at[:, pl.ds(start, lanes.stop - lanes.start)]
        own_w.append(pltpu.make_async_copy(part, wbuf.at[0, :, lanes], loc.at[3 + i]))
    for copy in own_w:
        copy.start()
    sources = list(small_in)
    for i in (1, 2):
        sources[i] = small_in[i].at[:, pl.ds(pl.multiple_of(z * 512, 512), 512)]
    own_small = [pltpu.make_async_copy(a, b, small_sem.at[i]) for i, (a, b) in enumerate(zip(sources, small_ref))]
    for copy in own_small:
        copy.start()
    own_s = pltpu.make_async_copy(state, sbuf, loc.at[1])
    own_s.start()
    own_wo = pltpu.make_async_copy(wout, wobuf.at[:, 0:128], loc.at[2])
    own_wo.start()

    own_tok.wait()
    for e in range(NX):
        squares = tokbuf[:, e].reshape(NZ * 32, 128).astype(f32)
        sqsend[e] = contract(jnp.ones((8, 128), f32), squares * squares, ((1,), (1,)), HIGHEST)[0:1]
    for copy in own_w:
        copy.wait()
    with jax.named_scope("barrier"):
        pl.semaphore_wait(barrier, len(near) + 1)

    for d in (2, 1, 3):
        go(remote(sqsend.at[lax.rem(x + d, NX)], sqrecv.at[d - 1], s_sq, r_sq, at_x(x + d)))

    mine, theirs = pl.ds(c * 4, 4), pl.ds(4 - c * 4, 4)
    for d in (2, 1, 3):
        go(remote(tokbuf.at[mine, lax.rem(x + d, NX)], xtok.at[d, mine], s_tok, tr.at[d - 1], at_x(x + d)))

    low, high = slice(0, 64), slice(64, 128)

    def direct(i):
        lanes = CHUNKS[i]
        go(remote(wbuf.at[0, :, lanes], wbuf.at[1, :, lanes], s_direct, wdr.at[i, 0], at_x(x + 1)))
        go(remote(wbuf.at[0, :, lanes], wbuf.at[3, :, lanes], s_direct, wdr.at[i, 1], at_x(x + 3)))

    def relay(i):
        lanes = CHUNKS[i]
        arrive(f"left{i}", wbuf.at[1, :, lanes], wdr.at[i, 0])
        go(remote(wbuf.at[1, low, lanes], wbuf.at[2, low, lanes], s_relay, wrr.at[i], at_x(x + 1)))
        arrive(f"right{i}", wbuf.at[3, :, lanes], wdr.at[i, 1])
        go(remote(wbuf.at[3, high, lanes], wbuf.at[2, high, lanes], s_relay, wrr.at[i], at_x(x + 3)))

    direct(0)
    direct(1)
    direct(2)

    def products(left, b, h):
        rows = pl.ds(pl.multiple_of(b * 8, 8), 8)
        pbuf[h, rows] = contract(left[h, rows], sbuf[b * NH + h], ((1,), (0,)), HIGHEST)

    def all_products(left, first, last):
        @pl.loop(first, last)
        def _(b):
            for h in range(NH):
                products(left, b, h)

    def every(ref, start, h):
        return ref[h, pl.ds(start, 8, stride=8)]

    def update_state(first, last):
        @pl.loop(first, last)
        def _(b):
            rows = pl.ds(pl.multiple_of(b * 8, 8), 8)
            for h in range(NH):
                added = contract(kold[h, rows], ubuf[h, rows], ((0,), (0,)), HIGHEST)
                matrix = sbuf[b * NH + h] * ebuf[h, rows][0:1] + added
                sbuf[b * NH + h] = matrix
                large = matrix.astype(bf16)
                halves[b * NH + h, 0:128] = large
                halves[b * NH + h, 128:256] = (matrix - large.astype(f32)).astype(bf16)

    def spread(k):
        pl.semaphore_signal(wave.at[k], inc=1, device_id=at_z(z + 1), device_id_type=MESH)
        pl.semaphore_signal(wave.at[k], inc=1, device_id=at_z(z - 1), device_id_type=MESH)

    spread(0)

    for copy in own_small:
        copy.wait()
    row = lax.broadcasted_iota(jnp.int32, (16, 32), 0)
    col = lax.broadcasted_iota(jnp.int32, (16, 32), 1) - tp * NH
    abw[...] = (
        contract(((row == col) & (row < NH)).astype(bf16), wdecay[...], ((1,), (0,)))
        + contract(((row == col + NH) & (row >= NH) & (row < 2 * NH)).astype(bf16), wbeta[...], ((1,), (0,)))
    ).astype(bf16)
    row = lax.broadcasted_iota(jnp.int32, (NX * NZ, 128), 0)
    for d in range(NX):
        here = row == z * NX + lax.rem(x + NX - d, NX)
        gainrow[d] = jnp.sum(jnp.where(here, gain[...], 0.0), axis=0, keepdims=True)
    pl.semaphore_wait(wave.at[0], 2)
    spread(1)
    keys = pkeys[...].astype(f32)
    kraw[...] = keys * lax.rsqrt(across(keys * keys) + epsilon)
    vraw[...] = pvalues[...].astype(f32)
    for h in range(NH):
        for t in range(NT):
            kold[h, pl.ds(t, 8, stride=8)] = kraw[pl.ds(h * NT + t, 8, stride=16)]
            kold[h, pl.ds(t + 4, 8, stride=8)] = jnp.zeros((8, 128), f32)
    kept = lax.rem(lax.broadcasted_iota(jnp.int32, (16, 8), 0), NT) < accepted[...]
    apart = lax.broadcasted_iota(jnp.int32, (16, 2048), 0) == lax.broadcasted_iota(jnp.int32, (16, 2048), 1) // 128
    apart = apart.astype(f32)
    gold[...] = contract(jnp.where(kept, plogs[...], 0.0), apart, ((0,), (0,)), HIGHEST)
    bold[...] = contract(jnp.where(kept, pbetas[...], 0.0), apart, ((0,), (0,)), HIGHEST)
    pl.semaphore_wait(wave.at[1], 2)
    spread(2)
    own_s.wait()
    all_products(kold, 0, 2)
    arrive("squares", sqrecv, r_sq)
    with jax.named_scope("wave"):
        pl.semaphore_wait(wave.at[2], 2)
    stsend[...] = ((sqsend[x] + sqrecv[0]) + sqrecv[1]) + sqrecv[2]
    for d in (4, 3, 5, 2, 6, 1, 7):
        go(remote(stsend, strecv.at[d - 1], s_stat, r_stat, at_z(z + d)))
    for d in (1, 3, 2):
        arrive(f"tokens{d}", xtok.at[d, mine], tr.at[d - 1])
        go(remote(xtok.at[d, mine], xtok.at[d, mine], s_twin, r_twin, twin))
    xtok[0] = tokbuf[:, x]
    relay(0)
    direct(3)
    all_products(kold, 2, NB)
    relay(1)
    direct(4)
    arrive("tokens", xtok.at[1:4, theirs], r_twin)

    for h in range(NH):
        keys = [every(kold, t, h) for t in range(NT)]
        written, decay = delta_rule(
            keys,
            [every(pbuf, t, h) for t in range(NT)],
            [vraw[pl.ds(h * NT + t, 8, stride=16)] for t in range(NT)],
            [gold[:, head(h * NT + t)] for t in range(NT)],
            [bold[:, head(h * NT + t)] for t in range(NT)],
        )
        for t in range(NT):
            last = written[t] if t == NT - 1 else decay[NT - 1, t] * written[t]
            ubuf[h, pl.ds(t, 8, stride=8)] = last
            ubuf[h, pl.ds(t + 4, 8, stride=8)] = jnp.zeros((8, 128), f32)
        ebuf[h, pl.ds(0, 8, stride=8)] = decay[NT - 1, -1]
    relay(2)
    direct(5)

    arrive("stats", strecv, r_stat)
    total = stsend[...]
    for d in range(NZ - 1):
        total = total + strecv[d]
    scale = lax.rsqrt(total * (1.0 / (NX * NZ * 128)) + epsilon)
    first_row = (lax.broadcasted_iota(jnp.int32, (8, 128), 0) == 0).astype(f32)
    scol[...] = contract(jnp.broadcast_to(scale, (8, 256)), first_row, ((0,), (0,)), HIGHEST).reshape(NZ, 32, 128)
    absend[...] = jnp.zeros((NZ, 8, 128), f32)
    for r in range(NZ):
        zz = dest(r)
        small = jnp.zeros((16, 32), f32)
        for d in range(NX):
            feature = lax.rem(x + NX - d, NX)
            normed = (xtok[d, zz].astype(f32) * scol[zz] * gainrow[d]).astype(bf16)
            nbuf[r * 32 : (r + 1) * 32, head(d)] = normed
            small = small + contract(abw[:, pl.ds(pl.multiple_of(feature * 128, 128), 128)], normed, ((1,), (1,)))
        absend[r, :, 0:32] = small[0:8]
    for r in range(1, NZ):
        go(remote(absend.at[r], abrecv.at[r - 1], s_small, r_small, at_z(dest(r))))
    def project(i):
        lanes = CHUNKS[i]
        arrive(f"far{i}", wbuf.at[2, :, lanes], wrr.at[i])
        rows = jnp.dot(
            nbuf[...], wbuf[:, :, lanes].reshape(512, lanes.stop - lanes.start), preferred_element_type=f32
        )
        if i % 2 == 0:
            yown[:, lanes] = rows[0:128]
            y1send[:, lanes] = rows[128:256].astype(bf16)
            other = z - side
        else:
            yown[0:32, lanes] = rows[0:32]
            yown[32:128, lanes] = rows[128:224]
            y1send[0:96, lanes] = rows[32:128].astype(bf16)
            y1send[96:128, lanes] = rows[224:256].astype(bf16)
            other = z + side
        go(remote(y1send.at[:, lanes], y1recv.at[:, lanes], s_y1, y1r.at[i], at_z(other)))

    def second_sum(i):
        lanes = CHUNKS[i]
        arrive(f"pair{i}", y1recv.at[:, lanes], y1r.at[i])
        rows = yown[:, lanes] + y1recv[:, lanes].astype(f32)
        yown[0:32, lanes] = rows[0:32]
        for j in range(3):
            y2send[j, :, lanes] = rows[32 * (j + 1) : 32 * (j + 2)].astype(bf16)
        way = side if i % 2 == 0 else -side
        for j in (3, 2, 1):
            go(remote(y2send.at[j - 1, :, lanes], y2recv.at[j - 1, :, lanes], s_y2, y2r.at[i], at_z(z + way * j)))

    def last_sum(i):
        lanes = CHUNKS[i]
        arrive(f"sum{i}", y2recv.at[:, :, lanes], y2r.at[i])

    def summed(m, h):
        lanes = head(m * NH + h)
        rows = yown[0:32, lanes]
        for j in range(3):
            rows = rows + y2recv[j, :, lanes].astype(f32)
        return rows

    project(0)
    relay(3)
    direct(6)
    project(1)
    update_state(0, 2)
    relay(4)
    direct(7)
    project(2)
    relay(5)
    update_state(2, 3)
    project(3)
    second_sum(0)
    relay(6)
    update_state(3, 4)
    second_sum(1)
    project(4)
    relay(7)
    own_wo.wait()
    for d in range(1, NX):
        go(remote(wobuf.at[:, 0:128], wobuf.at[:, d * 128 : (d + 1) * 128], s_wo, r_wo, at_x(x + d)))
    update_state(4, 5)
    second_sum(2)
    project(5)
    project(6)
    second_sum(3)
    project(7)
    second_sum(4)
    update_state(5, NB)

    arrive("small", abrecv, r_small)
    small = absend[0]
    for r in range(NZ - 1):
        small = small + abrecv[r]
    soft = jnp.maximum(small, 0.0) + jnp.log1p(jnp.exp(-jnp.abs(small)))
    which = lax.broadcasted_iota(jnp.int32, (8, 128), 0)
    lane = lax.broadcasted_iota(jnp.int32, (8, 32), 1)
    chosen = lane == tp * NH + lax.broadcasted_iota(jnp.int32, (8, 32), 0)
    rates = jnp.sum(jnp.where(chosen, rate[...], 0.0), axis=1, keepdims=True)
    small = jnp.where(which < NH, -rates * soft, 1.0 / (1.0 + jnp.exp(-small)))
    row = lax.broadcasted_iota(jnp.int32, (8, 512), 0)
    lane = lax.broadcasted_iota(jnp.int32, (8, 512), 1) // 128
    logs = contract(small, (row == lane).astype(f32), ((0,), (0,)), HIGHEST)
    strengths = contract(small, (row == lane + NH).astype(f32), ((0,), (0,)), HIGHEST)
    for h in range(NH):
        gnew[h] = logs[0:32, head(h)]
        bnew[h] = strengths[0:32, head(h)]

    def rows_of(ref, t, h):
        return ref[h, pl.ds(t, 8, stride=4)]

    def unit_rows(m, factor):
        for h in range(NH):
            v = silu(summed(m, h))
            tmp[h] = v * lax.rsqrt(across(v * v) + epsilon) * factor
            for t in range(NT):
                kq[h, pl.ds(m * 4 + t, 8, stride=8)] = rows_of(tmp, t, h)

    second_sum(5)
    second_sum(6)
    last_sum(0)
    last_sum(1)
    unit_rows(0, 1.0)
    second_sum(7)
    last_sum(2)
    last_sum(3)
    unit_rows(1, 128**-0.5)

    @pl.loop(0, NB)
    def _(b):
        rows = pl.ds(pl.multiple_of(b * 8, 8), 8)
        for h in range(NH):
            left = kq[h, rows]
            large = left.astype(bf16).astype(f32)
            left = jnp.concatenate(
                [jnp.concatenate([large, large], axis=1), jnp.concatenate([left - large, jnp.zeros_like(left)], axis=1)],
                axis=0,
            )
            both = contract(left.astype(bf16), halves[b * NH + h], ((1,), (0,)))
            pbuf[h, rows] = both[0:8] + both[8:16]

    last_sum(4)
    last_sum(5)
    for h in range(NH):
        vnew[h] = silu(summed(2, h))
    for h in range(NH):
        keys = [every(kq, t, h) for t in range(NT)]
        written, decay = delta_rule(
            keys,
            [every(pbuf, t, h) for t in range(NT)],
            [rows_of(vnew, t, h) for t in range(NT)],
            [rows_of(gnew, t, h) for t in range(NT)],
            [rows_of(bnew, t, h) for t in range(NT)],
        )
        for t in range(NT):
            query = every(kq, 4 + t, h)
            attended = decay[t, -1] * every(pbuf, 4 + t, h) + across(keys[t] * query) * written[t]
            for i in range(t):
                attended = attended + decay[t, i] * across(keys[i] * query) * written[i]
            scaled = attended * lax.rsqrt(across(attended * attended) * (1.0 / 128) + epsilon)
            hout[h, pl.ds(t, 8, stride=4)] = scaled * hgain[...]

    for g in range(2):
        last_sum(6 + g)
        for h in (2 * g, 2 * g + 1):
            hsend[g, :, head(h - 2 * g)] = (hout[h] * silu(summed(3, h))).astype(bf16)
        for d in (4, 3, 5, 2, 6, 1, 7):
            go(remote(hsend.at[g], hz.at[g, d], hs.at[g], hr.at[g], at_z(z + d)))
        hz[g, 0] = hsend[g]

    arrive("wout", wobuf.at[:, 128:512], r_wo)
    arrive("heads0", hz.at[0, 1:8], hr.at[0])
    terms = jnp.dot(hz[0].reshape(256, 256), wobuf[0:256], preferred_element_type=f32)
    arrive("heads1", hz.at[1, 1:8], hr.at[1])
    terms = terms + jnp.dot(hz[1].reshape(256, 256), wobuf[256:512], preferred_element_type=f32)
    for d in range(NZ):
        zz = lax.rem(z + NZ - d, NZ)
        p3[lax.rem(zz, 2) * NY + zz // 2] = terms[d * 32 : (d + 1) * 32]
    go(remote(p3.at[pl.ds((1 - c) * NY, NY)], d2d, s_d2d, r_d2d, twin))
    arrive("twin", d2d, r_d2d)
    for j in range(NY):
        rows = p3[c * NY + j] + d2d[j]
        for e in range(NX):
            psend[j * NX + e] = rows[:, head(e)].astype(bf16)
    for ey, ex in (
        (2, 2), (2, 1), (2, 3), (1, 2), (3, 2), (2, 0), (0, 2), (1, 1), (1, 3), (3, 1), (3, 3), (1, 0), (3, 0), (0, 1), (0, 3),
    ):
        there = {"kv": z * NX + lax.rem(x + NX - ex, NX), "tp": lax.rem(y + ey, NY) * 2 + c}
        go(remote(psend.at[lax.rem(y + ey, NY) * NX + ex], precv.at[ey * NX + ex], s_part, r_part, there))
    own_part = p3[c * NY + y, :, 0:128] + d2d[y, :, 0:128]
    arrive("parts", precv.at[1:16], r_part)
    for ex in range(NX):
        total = own_part if ex == 0 else precv[ex].astype(f32)
        for ey in range(1, NY):
            total = total + precv[ey * NX + ex].astype(f32)
        mixed[lax.rem(x + ex, NX)] = total.astype(bf16)
    for ref, sem in (
        (xtok.at[1:4, mine], s_tok), (wbuf.at[0:2], s_direct), (wbuf.at[0], s_relay), (sqrecv, s_sq), (strecv, s_stat), (abrecv, s_small),
        (y1send, s_y1), (y2send, s_y2), (wobuf.at[:, 128:512], s_wo), (xtok.at[1:4, mine], s_twin), (d2d, s_d2d),
        (hz.at[0, 1:8], hs.at[0]), (hz.at[1, 1:8], hs.at[1]), (precv.at[1:16], s_part),
    ):
        arrive("drain", ref, sem)


def fused(*operands):
    anywhere = pl.BlockSpec(memory_space=pl.ANY)
    vmem = pl.BlockSpec(memory_space=pltpu.VMEM)
    dma = pltpu.SemaphoreType.DMA
    scratch = [
        pltpu.VMEM((NX * NZ, 128), f32),
        pltpu.VMEM((32, 512), bf16),
        pltpu.VMEM((32, 512), bf16),
        pltpu.VMEM((128, 128), bf16),
        pltpu.VMEM((128, 128), bf16),
        pltpu.VMEM((16, 8), f32),
        pltpu.VMEM((16, 8), f32),
        pltpu.VMEM((1, 8), jnp.int32),
        pltpu.VMEM((1, 32), f32),
        pltpu.VMEM((1, 128), f32),
        dma((10,)),
        pltpu.VMEM((128, 128), f32),
        pltpu.VMEM((128, 128), f32),
        pltpu.VMEM((NH, 64, 128), f32),
        pltpu.VMEM((8, 2048), f32),
        pltpu.VMEM((8, 2048), f32),
        pltpu.VMEM((16, 512), bf16),
        pltpu.VMEM((NX, 1, 128), f32),
        pltpu.VMEM((NZ, NX, 32, 128), bf16),
        pltpu.VMEM((NX, NZ, 32, 128), bf16),
        pltpu.VMEM((NX, 128, 2048), bf16),
        pltpu.VMEM((NX, 1, 256), f32),
        pltpu.VMEM((NX - 1, 1, 256), f32),
        pltpu.VMEM((1, 256), f32),
        pltpu.VMEM((NZ - 1, 1, 256), f32),
        pltpu.VMEM((NZ, 32, 128), f32),
        pltpu.VMEM((256, 512), bf16),
        pltpu.VMEM((NZ, 8, 128), f32),
        pltpu.VMEM((NZ - 1, 8, 128), f32),
        pltpu.VMEM((128, 2048), f32),
        pltpu.VMEM((128, 2048), bf16),
        pltpu.VMEM((128, 2048), bf16),
        pltpu.VMEM((3, 32, 2048), bf16),
        pltpu.VMEM((3, 32, 2048), bf16),
        pltpu.VMEM((512, 512), bf16),
        pltpu.VMEM((NB * NH, 256, 128), bf16),
        pltpu.VMEM((NH, 64, 128), f32),
        pltpu.VMEM((NH, 64, 128), f32),
        pltpu.VMEM((NH, 64, 128), f32),
        pltpu.VMEM((NH, 32, 128), f32),
        pltpu.VMEM((NH, 64, 128), f32),
        pltpu.VMEM((NH, 32, 128), f32),
        pltpu.VMEM((NH, 32, 128), f32),
        pltpu.VMEM((NH, 32, 128), f32),
        pltpu.VMEM((NH, 32, 128), f32),
        pltpu.VMEM((2, 32, 256), bf16),
        pltpu.VMEM((2, NZ, 32, 256), bf16),
        pltpu.VMEM((NZ, 32, 512), f32),
        pltpu.VMEM((NY, 32, 512), f32),
        pltpu.VMEM((NY * NX, 32, 128), bf16),
        pltpu.VMEM((NY * NX, 32, 128), bf16),
        dma((3 + NC,)),
        dma((3,)),
        dma((NC, 2)),
        dma((NC,)),
        dma((NC,)),
        dma((NC,)),
        dma((2,)),
        dma((2,)),
        dma((12,)),
        dma((7,)),
        pltpu.SemaphoreType.REGULAR((3,)),
    ]
    return pl.pallas_call(
        kernel,
        out_shape=(
            pltpu.VMEM((NX, 32, 128), bf16),
            pltpu.VMEM((NB * NH, 128, 128), f32),
        ),
        in_specs=[anywhere] * 17,
        out_specs=(vmem, vmem),
        scratch_shapes=scratch,
        compiler_params=pltpu.CompilerParams(collective_id=0, has_side_effects=True),
        name="step",
    )(*operands)


def to_hbm(mixed, carried):
    parts = 4

    def body(mixed, carried, mixed_out, carried_out, sems):
        size = carried.shape[0] // parts
        copies = [pltpu.make_async_copy(mixed, mixed_out, sems.at[parts])]
        for i in range(parts):
            rows = pl.ds(i * size, size)
            copies.append(pltpu.make_async_copy(carried.at[rows], carried_out.at[rows], sems.at[i]))
        for copy in copies:
            copy.start()
        for copy in copies:
            copy.wait()

    vmem, hbm = pl.BlockSpec(memory_space=pltpu.VMEM), pl.BlockSpec(memory_space=pltpu.HBM)
    return pl.pallas_call(
        body,
        out_shape=tuple(pltpu.HBM(a.shape, a.dtype) for a in (mixed, carried)),
        in_specs=[vmem, vmem],
        out_specs=(hbm, hbm),
        scratch_shapes=[pltpu.SemaphoreType.DMA((parts + 1,))],
        name="to_hbm",
    )(pltpu.with_memory_space_constraint(mixed, pltpu.VMEM), pltpu.with_memory_space_constraint(carried, pltpu.VMEM))


def per_device(
    tokens,
    norm_gain,
    w_query,
    w_key,
    w_value,
    w_gate,
    w_decay,
    w_beta,
    decay_rate,
    head_gain,
    w_out,
    state,
    prev_keys,
    prev_values,
    prev_log_decay,
    prev_beta,
    accepted,
):
    mixed, carried = fused(
        tokens.reshape(NZ, NX, 32, 128), w_key, w_query, w_value, w_gate, w_out,
        state.reshape(NB * NH, 128, 128), norm_gain.reshape(NX * NZ, 128), w_decay.T, w_beta.T,
        prev_keys.reshape(128, 128), prev_values.reshape(128, 128),
        prev_log_decay.transpose(1, 2, 0).reshape(16, NB), prev_beta.transpose(1, 2, 0).reshape(16, NB),
        accepted.reshape(1, NB), decay_rate.reshape(1, 32), head_gain.reshape(1, 128),
    )
    mixed, carried = to_hbm(mixed, carried)
    return mixed.reshape(32, NT, 128), carried.reshape(NB, NH, 128, 128)


def solution(mesh):
    placed = (
        P(None, None, "kv"),
        P(),
        P("kv", "tp"),
        P("kv", "tp"),
        P("kv", "tp"),
        P("kv", "tp"),
        P(),
        P(),
        P(),
        P(),
        P("tp", "kv"),
        P("kv", "tp", None, None),
        P("kv", "tp", None, None),
        P("kv", "tp", None, None),
        P("kv", "tp", None),
        P("kv", "tp", None),
        P("kv"),
    )
    return jax.shard_map(
        per_device,
        mesh=mesh,
        in_specs=placed,
        out_specs=(P("tp", None, "kv"), P("kv", "tp", None, None)),
        check_vma=False,
    )
```

```python
import jax
import jax.numpy as jnp
from jax import lax
from jax.experimental import pallas as pl
from jax.experimental.pallas import tpu as pltpu
from jax.sharding import PartitionSpec as P

MESH = pl.DeviceIdType.MESH
HIGHEST = lax.Precision.HIGHEST
epsilon = 1e-06

NZ, NX, NY, NT, NB, NH = 8, 4, 4, 4, 8, 4
f32, bf16 = jnp.float32, jnp.bfloat16
NC, WIDE = 8, 256
CHUNKS = tuple(slice(i * WIDE, (i + 1) * WIDE) for i in range(NC))


def contract(a, b, dims, precision=None):
    return lax.dot_general(a, b, (dims, ((), ())), precision=precision, preferred_element_type=f32)


def silu(v):
    return v / (1.0 + jnp.exp(-v))


def head(h):
    return slice(h * 128, (h + 1) * 128)


def across(v):
    return jnp.sum(v, axis=-1, keepdims=True)


def delta_rule(keys, predicted, values, logs, betas):
    decay = {}
    for t in range(NT):
        total = logs[t]
        decay[t, t] = None
        for i in range(t - 1, -1, -1):
            decay[t, i] = jnp.exp(total)
            total = total + logs[i]
        decay[t, -1] = jnp.exp(total)
    written = []
    for t in range(NT):
        expected = decay[t, -1] * predicted[t]
        for i in range(t):
            expected = expected + decay[t, i] * across(keys[i] * keys[t]) * written[i]
        written.append(betas[t] * (values[t] - expected))
    return written, decay


def kernel(
    tok, wkey, wquery, wvalue, wgate, wout, state, *rest
):
    small_in, (mixed, sbuf, *rest) = rest[:10], rest[10:]
    small_ref, rest = rest[:10], rest[10:]
    gain, wdecay, wbeta, pkeys, pvalues, plogs, pbetas, accepted, rate, hgain = small_ref
    (
    small_sem, kraw, vraw, kold, gold, bold, abw, gainrow, tokbuf, xtok, wbuf, sqsend, sqrecv, stsend, strecv, scol, nbuf, absend, abrecv,
    yown, y1send, y1recv, y2send, y2recv, wobuf, halves, pbuf, ubuf, ebuf, tmp, kq, gnew, bnew, vnew, hout,
    hsend, hz, p3, d2d, psend, precv,
    loc, tr, wdr, wrr, y1r, y2r, hr, hs, sent, got, wave,
    ) = rest
    s_sq, s_tok, s_direct, s_relay, s_stat, s_small, s_y1, s_y2, s_wo, s_twin, s_d2d, s_part = [sent.at[i] for i in range(12)]
    r_sq, r_stat, r_small, r_wo, r_twin, r_d2d, r_part = [got.at[i] for i in range(7)]
    kv, tp = lax.axis_index("kv"), lax.axis_index("tp")
    z, x, y, c = kv // NX, lax.rem(kv, NX), tp // 2, lax.rem(tp, 2)
    side = 2 * lax.rem(z, 2) - 1
    weights = (wkey, wquery, wvalue, wgate)

    def at_z(zz):
        return {"kv": lax.rem(zz + 2 * NZ, NZ) * NX + x}

    def at_x(xx):
        return {"kv": z * NX + lax.rem(xx + NX, NX)}

    def dest(r):
        off = side * r if r < 4 else -side * (r - 3)
        return lax.rem(z + off + 2 * NZ, NZ)

    def remote(src, dst, send, recv, device):
        return pltpu.make_async_remote_copy(
            src_ref=src, dst_ref=dst, send_sem=send, recv_sem=recv, device_id=device, device_id_type=MESH
        )

    twin = {"tp": tp + 1 - 2 * c}

    def go(copy):
        copy.start()
        return copy

    def arrive(name, ref, sem):
        with jax.named_scope(name):
            pltpu.make_async_copy(ref, ref, sem).wait()

    barrier = pltpu.get_barrier_semaphore()
    near = [at_x(x + d) for d in (1, 3, 2)] + [at_z(z + 1), at_z(z - 1)]
    near += [{"tp": lax.rem(y + d, NY) * 2 + c} for d in (1, 3, 2)]
    for there in near:
        pl.semaphore_signal(barrier, inc=1, device_id=there, device_id_type=MESH)
    pl.semaphore_signal(barrier, inc=1, device_id=twin, device_id_type=MESH)

    own_tok = pltpu.make_async_copy(tok, tokbuf, loc.at[0])
    own_tok.start()
    own_w = []
    for i, lanes in enumerate(CHUNKS):
        m, start = lanes.start // 512, lanes.start % 512
        part = weights[m].at[:, pl.ds(start, lanes.stop - lanes.start)]
        own_w.append(pltpu.make_async_copy(part, wbuf.at[0, :, lanes], loc.at[3 + i]))
    for copy in own_w:
        copy.start()
    sources = list(small_in)
    for i in (1, 2):
        sources[i] = small_in[i].at[:, pl.ds(pl.multiple_of(z * 512, 512), 512)]
    own_small = [pltpu.make_async_copy(a, b, small_sem.at[i]) for i, (a, b) in enumerate(zip(sources, small_ref))]
    for copy in own_small:
        copy.start()
    own_s = pltpu.make_async_copy(state, sbuf, loc.at[1])
    own_s.start()
    own_wo = pltpu.make_async_copy(wout, wobuf.at[:, 0:128], loc.at[2])
    own_wo.start()

    own_tok.wait()
    for e in range(NX):
        squares = tokbuf[:, e].reshape(NZ * 32, 128).astype(f32)
        sqsend[e] = contract(jnp.ones((8, 128), f32), squares * squares, ((1,), (1,)), HIGHEST)[0:1]
    for copy in own_w:
        copy.wait()
    with jax.named_scope("barrier"):
        pl.semaphore_wait(barrier, len(near) + 1)

    for d in (2, 1, 3):
        go(remote(sqsend.at[lax.rem(x + d, NX)], sqrecv.at[d - 1], s_sq, r_sq, at_x(x + d)))

    mine, theirs = pl.ds(c * 4, 4), pl.ds(4 - c * 4, 4)
    for d in (2, 1, 3):
        go(remote(tokbuf.at[mine, lax.rem(x + d, NX)], xtok.at[d, mine], s_tok, tr.at[d - 1], at_x(x + d)))

    low, high = slice(0, 64), slice(64, 128)

    def direct(i):
        lanes = CHUNKS[i]
        go(remote(wbuf.at[0, :, lanes], wbuf.at[1, :, lanes], s_direct, wdr.at[i, 0], at_x(x + 1)))
        go(remote(wbuf.at[0, :, lanes], wbuf.at[3, :, lanes], s_direct, wdr.at[i, 1], at_x(x + 3)))

    def relay(i):
        lanes = CHUNKS[i]
        arrive(f"left{i}", wbuf.at[1, :, lanes], wdr.at[i, 0])
        go(remote(wbuf.at[1, low, lanes], wbuf.at[2, low, lanes], s_relay, wrr.at[i], at_x(x + 1)))
        arrive(f"right{i}", wbuf.at[3, :, lanes], wdr.at[i, 1])
        go(remote(wbuf.at[3, high, lanes], wbuf.at[2, high, lanes], s_relay, wrr.at[i], at_x(x + 3)))

    direct(0)
    direct(1)
    direct(2)

    def products(left, b, h):
        rows = pl.ds(pl.multiple_of(b * 8, 8), 8)
        pbuf[h, rows] = contract(left[h, rows], sbuf[b * NH + h], ((1,), (0,)), HIGHEST)

    def all_products(left, first, last):
        @pl.loop(first, last)
        def _(b):
            for h in range(NH):
                products(left, b, h)

    def every(ref, start, h):
        return ref[h, pl.ds(start, 8, stride=8)]

    def update_state(first, last):
        @pl.loop(first, last)
        def _(b):
            rows = pl.ds(pl.multiple_of(b * 8, 8), 8)
            for h in range(NH):
                added = contract(kold[h, rows], ubuf[h, rows], ((0,), (0,)), HIGHEST)
                matrix = sbuf[b * NH + h] * ebuf[h, rows][0:1] + added
                sbuf[b * NH + h] = matrix
                large = matrix.astype(bf16)
                halves[b * NH + h, 0:128] = large
                halves[b * NH + h, 128:256] = (matrix - large.astype(f32)).astype(bf16)

    def spread(k):
        pl.semaphore_signal(wave.at[k], inc=1, device_id=at_z(z + 1), device_id_type=MESH)
        pl.semaphore_signal(wave.at[k], inc=1, device_id=at_z(z - 1), device_id_type=MESH)

    spread(0)

    for copy in own_small:
        copy.wait()
    row = lax.broadcasted_iota(jnp.int32, (16, 32), 0)
    col = lax.broadcasted_iota(jnp.int32, (16, 32), 1) - tp * NH
    abw[...] = (
        contract(((row == col) & (row < NH)).astype(bf16), wdecay[...], ((1,), (0,)))
        + contract(((row == col + NH) & (row >= NH) & (row < 2 * NH)).astype(bf16), wbeta[...], ((1,), (0,)))
    ).astype(bf16)
    row = lax.broadcasted_iota(jnp.int32, (NX * NZ, 128), 0)
    for d in range(NX):
        here = row == z * NX + lax.rem(x + NX - d, NX)
        gainrow[d] = jnp.sum(jnp.where(here, gain[...], 0.0), axis=0, keepdims=True)
    pl.semaphore_wait(wave.at[0], 2)
    spread(1)
    keys = pkeys[...].astype(f32)
    kraw[...] = keys * lax.rsqrt(across(keys * keys) + epsilon)
    vraw[...] = pvalues[...].astype(f32)
    for h in range(NH):
        for t in range(NT):
            kold[h, pl.ds(t, 8, stride=8)] = kraw[pl.ds(h * NT + t, 8, stride=16)]
            kold[h, pl.ds(t + 4, 8, stride=8)] = jnp.zeros((8, 128), f32)
    kept = lax.rem(lax.broadcasted_iota(jnp.int32, (16, 8), 0), NT) < accepted[...]
    apart = lax.broadcasted_iota(jnp.int32, (16, 2048), 0) == lax.broadcasted_iota(jnp.int32, (16, 2048), 1) // 128
    apart = apart.astype(f32)
    gold[...] = contract(jnp.where(kept, plogs[...], 0.0), apart, ((0,), (0,)), HIGHEST)
    bold[...] = contract(jnp.where(kept, pbetas[...], 0.0), apart, ((0,), (0,)), HIGHEST)
    pl.semaphore_wait(wave.at[1], 2)
    spread(2)
    own_s.wait()
    all_products(kold, 0, 2)
    arrive("squares", sqrecv, r_sq)
    with jax.named_scope("wave"):
        pl.semaphore_wait(wave.at[2], 2)
    stsend[...] = ((sqsend[x] + sqrecv[0]) + sqrecv[1]) + sqrecv[2]
    for d in (4, 3, 5, 2, 6, 1, 7):
        go(remote(stsend, strecv.at[d - 1], s_stat, r_stat, at_z(z + d)))
    for d in (1, 3, 2):
        arrive(f"tokens{d}", xtok.at[d, mine], tr.at[d - 1])
        go(remote(xtok.at[d, mine], xtok.at[d, mine], s_twin, r_twin, twin))
    xtok[0] = tokbuf[:, x]
    relay(0)
    direct(3)
    all_products(kold, 2, NB)
    relay(1)
    direct(4)
    arrive("tokens", xtok.at[1:4, theirs], r_twin)

    for h in range(NH):
        keys = [every(kold, t, h) for t in range(NT)]
        written, decay = delta_rule(
            keys,
            [every(pbuf, t, h) for t in range(NT)],
            [vraw[pl.ds(h * NT + t, 8, stride=16)] for t in range(NT)],
            [gold[:, head(h * NT + t)] for t in range(NT)],
            [bold[:, head(h * NT + t)] for t in range(NT)],
        )
        for t in range(NT):
            last = written[t] if t == NT - 1 else decay[NT - 1, t] * written[t]
            ubuf[h, pl.ds(t, 8, stride=8)] = last
            ubuf[h, pl.ds(t + 4, 8, stride=8)] = jnp.zeros((8, 128), f32)
        ebuf[h, pl.ds(0, 8, stride=8)] = decay[NT - 1, -1]
    relay(2)
    direct(5)

    arrive("stats", strecv, r_stat)
    total = stsend[...]
    for d in range(NZ - 1):
        total = total + strecv[d]
    scale = lax.rsqrt(total * (1.0 / (NX * NZ * 128)) + epsilon)
    first_row = (lax.broadcasted_iota(jnp.int32, (8, 128), 0) == 0).astype(f32)
    scol[...] = contract(jnp.broadcast_to(scale, (8, 256)), first_row, ((0,), (0,)), HIGHEST).reshape(NZ, 32, 128)
    absend[...] = jnp.zeros((NZ, 8, 128), f32)
    for r in range(NZ):
        zz = dest(r)
        small = jnp.zeros((16, 32), f32)
        for d in range(NX):
            feature = lax.rem(x + NX - d, NX)
            normed = (xtok[d, zz].astype(f32) * scol[zz] * gainrow[d]).astype(bf16)
            nbuf[r * 32 : (r + 1) * 32, head(d)] = normed
            small = small + contract(abw[:, pl.ds(pl.multiple_of(feature * 128, 128), 128)], normed, ((1,), (1,)))
        absend[r, :, 0:32] = small[0:8]
    for r in range(1, NZ):
        go(remote(absend.at[r], abrecv.at[r - 1], s_small, r_small, at_z(dest(r))))
    def project(i):
        lanes = CHUNKS[i]
        arrive(f"far{i}", wbuf.at[2, :, lanes], wrr.at[i])
        rows = jnp.dot(
            nbuf[...], wbuf[:, :, lanes].reshape(512, lanes.stop - lanes.start), preferred_element_type=f32
        )
        if i % 2 == 0:
            yown[:, lanes] = rows[0:128]
            y1send[:, lanes] = rows[128:256].astype(bf16)
            other = z - side
        else:
            yown[0:32, lanes] = rows[0:32]
            yown[32:128, lanes] = rows[128:224]
            y1send[0:96, lanes] = rows[32:128].astype(bf16)
            y1send[96:128, lanes] = rows[224:256].astype(bf16)
            other = z + side
        go(remote(y1send.at[:, lanes], y1recv.at[:, lanes], s_y1, y1r.at[i], at_z(other)))

    def second_sum(i):
        lanes = CHUNKS[i]
        arrive(f"pair{i}", y1recv.at[:, lanes], y1r.at[i])
        rows = yown[:, lanes] + y1recv[:, lanes].astype(f32)
        yown[0:32, lanes] = rows[0:32]
        for j in range(3):
            y2send[j, :, lanes] = rows[32 * (j + 1) : 32 * (j + 2)].astype(bf16)
        way = side if i % 2 == 0 else -side
        for j in (3, 2, 1):
            go(remote(y2send.at[j - 1, :, lanes], y2recv.at[j - 1, :, lanes], s_y2, y2r.at[i], at_z(z + way * j)))

    def last_sum(i):
        lanes = CHUNKS[i]
        arrive(f"sum{i}", y2recv.at[:, :, lanes], y2r.at[i])

    def summed(m, h):
        lanes = head(m * NH + h)
        rows = yown[0:32, lanes]
        for j in range(3):
            rows = rows + y2recv[j, :, lanes].astype(f32)
        return rows

    project(0)
    relay(3)
    direct(6)
    project(1)
    update_state(0, 2)
    relay(4)
    direct(7)
    project(2)
    relay(5)
    project(3)
    second_sum(0)
    relay(6)
    update_state(2, 4)
    second_sum(1)
    project(4)
    relay(7)
    own_wo.wait()
    for d in range(1, NX):
        go(remote(wobuf.at[:, 0:128], wobuf.at[:, d * 128 : (d + 1) * 128], s_wo, r_wo, at_x(x + d)))
    update_state(4, 5)
    second_sum(2)
    project(5)
    project(6)
    second_sum(3)
    project(7)
    second_sum(4)
    update_state(5, NB)

    arrive("small", abrecv, r_small)
    small = absend[0]
    for r in range(NZ - 1):
        small = small + abrecv[r]
    soft = jnp.maximum(small, 0.0) + jnp.log1p(jnp.exp(-jnp.abs(small)))
    which = lax.broadcasted_iota(jnp.int32, (8, 128), 0)
    lane = lax.broadcasted_iota(jnp.int32, (8, 32), 1)
    chosen = lane == tp * NH + lax.broadcasted_iota(jnp.int32, (8, 32), 0)
    rates = jnp.sum(jnp.where(chosen, rate[...], 0.0), axis=1, keepdims=True)
    small = jnp.where(which < NH, -rates * soft, 1.0 / (1.0 + jnp.exp(-small)))
    row = lax.broadcasted_iota(jnp.int32, (8, 512), 0)
    lane = lax.broadcasted_iota(jnp.int32, (8, 512), 1) // 128
    logs = contract(small, (row == lane).astype(f32), ((0,), (0,)), HIGHEST)
    strengths = contract(small, (row == lane + NH).astype(f32), ((0,), (0,)), HIGHEST)
    for h in range(NH):
        gnew[h] = logs[0:32, head(h)]
        bnew[h] = strengths[0:32, head(h)]

    def rows_of(ref, t, h):
        return ref[h, pl.ds(t, 8, stride=4)]

    def unit_rows(m, factor):
        for h in range(NH):
            v = silu(summed(m, h))
            tmp[h] = v * lax.rsqrt(across(v * v) + epsilon) * factor
            for t in range(NT):
                kq[h, pl.ds(m * 4 + t, 8, stride=8)] = rows_of(tmp, t, h)

    second_sum(5)
    second_sum(6)
    last_sum(0)
    last_sum(1)
    unit_rows(0, 1.0)
    second_sum(7)
    last_sum(2)
    last_sum(3)
    unit_rows(1, 128**-0.5)

    @pl.loop(0, NB)
    def _(b):
        rows = pl.ds(pl.multiple_of(b * 8, 8), 8)
        for h in range(NH):
            left = kq[h, rows]
            large = left.astype(bf16).astype(f32)
            left = jnp.concatenate(
                [jnp.concatenate([large, large], axis=1), jnp.concatenate([left - large, jnp.zeros_like(left)], axis=1)],
                axis=0,
            )
            both = contract(left.astype(bf16), halves[b * NH + h], ((1,), (0,)))
            pbuf[h, rows] = both[0:8] + both[8:16]

    last_sum(4)
    last_sum(5)
    for h in range(NH):
        vnew[h] = silu(summed(2, h))
    for h in range(NH):
        keys = [every(kq, t, h) for t in range(NT)]
        written, decay = delta_rule(
            keys,
            [every(pbuf, t, h) for t in range(NT)],
            [rows_of(vnew, t, h) for t in range(NT)],
            [rows_of(gnew, t, h) for t in range(NT)],
            [rows_of(bnew, t, h) for t in range(NT)],
        )
        for t in range(NT):
            query = every(kq, 4 + t, h)
            attended = decay[t, -1] * every(pbuf, 4 + t, h) + across(keys[t] * query) * written[t]
            for i in range(t):
                attended = attended + decay[t, i] * across(keys[i] * query) * written[i]
            scaled = attended * lax.rsqrt(across(attended * attended) * (1.0 / 128) + epsilon)
            hout[h, pl.ds(t, 8, stride=4)] = scaled * hgain[...]

    for g in range(2):
        last_sum(6 + g)
        for h in (2 * g, 2 * g + 1):
            hsend[g, :, head(h - 2 * g)] = (hout[h] * silu(summed(3, h))).astype(bf16)
        for d in (4, 3, 5, 2, 6, 1, 7):
            go(remote(hsend.at[g], hz.at[g, d], hs.at[g], hr.at[g], at_z(z + d)))
        hz[g, 0] = hsend[g]

    arrive("wout", wobuf.at[:, 128:512], r_wo)
    arrive("heads0", hz.at[0, 1:8], hr.at[0])
    terms = jnp.dot(hz[0].reshape(256, 256), wobuf[0:256], preferred_element_type=f32)
    arrive("heads1", hz.at[1, 1:8], hr.at[1])
    terms = terms + jnp.dot(hz[1].reshape(256, 256), wobuf[256:512], preferred_element_type=f32)
    for d in range(NZ):
        zz = lax.rem(z + NZ - d, NZ)
        p3[lax.rem(zz, 2) * NY + zz // 2] = terms[d * 32 : (d + 1) * 32]
    go(remote(p3.at[pl.ds((1 - c) * NY, NY)], d2d, s_d2d, r_d2d, twin))
    arrive("twin", d2d, r_d2d)
    for j in range(NY):
        rows = p3[c * NY + j] + d2d[j]
        for e in range(NX):
            psend[j * NX + e] = rows[:, head(e)].astype(bf16)
    for ey, ex in (
        (2, 2), (2, 1), (2, 3), (1, 2), (3, 2), (2, 0), (0, 2), (1, 1), (1, 3), (3, 1), (3, 3), (1, 0), (3, 0), (0, 1), (0, 3),
    ):
        there = {"kv": z * NX + lax.rem(x + NX - ex, NX), "tp": lax.rem(y + ey, NY) * 2 + c}
        go(remote(psend.at[lax.rem(y + ey, NY) * NX + ex], precv.at[ey * NX + ex], s_part, r_part, there))
    own_part = p3[c * NY + y, :, 0:128] + d2d[y, :, 0:128]
    arrive("parts", precv.at[1:16], r_part)
    for ex in range(NX):
        total = own_part if ex == 0 else precv[ex].astype(f32)
        for ey in range(1, NY):
            total = total + precv[ey * NX + ex].astype(f32)
        mixed[lax.rem(x + ex, NX)] = total.astype(bf16)
    for ref, sem in (
        (xtok.at[1:4, mine], s_tok), (wbuf.at[0:2], s_direct), (wbuf.at[0], s_relay), (sqrecv, s_sq), (strecv, s_stat), (abrecv, s_small),
        (y1send, s_y1), (y2send, s_y2), (wobuf.at[:, 128:512], s_wo), (xtok.at[1:4, mine], s_twin), (d2d, s_d2d),
        (hz.at[0, 1:8], hs.at[0]), (hz.at[1, 1:8], hs.at[1]), (precv.at[1:16], s_part),
    ):
        arrive("drain", ref, sem)


def fused(*operands):
    anywhere = pl.BlockSpec(memory_space=pl.ANY)
    vmem = pl.BlockSpec(memory_space=pltpu.VMEM)
    dma = pltpu.SemaphoreType.DMA
    scratch = [
        pltpu.VMEM((NX * NZ, 128), f32),
        pltpu.VMEM((32, 512), bf16),
        pltpu.VMEM((32, 512), bf16),
        pltpu.VMEM((128, 128), bf16),
        pltpu.VMEM((128, 128), bf16),
        pltpu.VMEM((16, 8), f32),
        pltpu.VMEM((16, 8), f32),
        pltpu.VMEM((1, 8), jnp.int32),
        pltpu.VMEM((1, 32), f32),
        pltpu.VMEM((1, 128), f32),
        dma((10,)),
        pltpu.VMEM((128, 128), f32),
        pltpu.VMEM((128, 128), f32),
        pltpu.VMEM((NH, 64, 128), f32),
        pltpu.VMEM((8, 2048), f32),
        pltpu.VMEM((8, 2048), f32),
        pltpu.VMEM((16, 512), bf16),
        pltpu.VMEM((NX, 1, 128), f32),
        pltpu.VMEM((NZ, NX, 32, 128), bf16),
        pltpu.VMEM((NX, NZ, 32, 128), bf16),
        pltpu.VMEM((NX, 128, 2048), bf16),
        pltpu.VMEM((NX, 1, 256), f32),
        pltpu.VMEM((NX - 1, 1, 256), f32),
        pltpu.VMEM((1, 256), f32),
        pltpu.VMEM((NZ - 1, 1, 256), f32),
        pltpu.VMEM((NZ, 32, 128), f32),
        pltpu.VMEM((256, 512), bf16),
        pltpu.VMEM((NZ, 8, 128), f32),
        pltpu.VMEM((NZ - 1, 8, 128), f32),
        pltpu.VMEM((128, 2048), f32),
        pltpu.VMEM((128, 2048), bf16),
        pltpu.VMEM((128, 2048), bf16),
        pltpu.VMEM((3, 32, 2048), bf16),
        pltpu.VMEM((3, 32, 2048), bf16),
        pltpu.VMEM((512, 512), bf16),
        pltpu.VMEM((NB * NH, 256, 128), bf16),
        pltpu.VMEM((NH, 64, 128), f32),
        pltpu.VMEM((NH, 64, 128), f32),
        pltpu.VMEM((NH, 64, 128), f32),
        pltpu.VMEM((NH, 32, 128), f32),
        pltpu.VMEM((NH, 64, 128), f32),
        pltpu.VMEM((NH, 32, 128), f32),
        pltpu.VMEM((NH, 32, 128), f32),
        pltpu.VMEM((NH, 32, 128), f32),
        pltpu.VMEM((NH, 32, 128), f32),
        pltpu.VMEM((2, 32, 256), bf16),
        pltpu.VMEM((2, NZ, 32, 256), bf16),
        pltpu.VMEM((NZ, 32, 512), f32),
        pltpu.VMEM((NY, 32, 512), f32),
        pltpu.VMEM((NY * NX, 32, 128), bf16),
        pltpu.VMEM((NY * NX, 32, 128), bf16),
        dma((3 + NC,)),
        dma((3,)),
        dma((NC, 2)),
        dma((NC,)),
        dma((NC,)),
        dma((NC,)),
        dma((2,)),
        dma((2,)),
        dma((12,)),
        dma((7,)),
        pltpu.SemaphoreType.REGULAR((3,)),
    ]
    return pl.pallas_call(
        kernel,
        out_shape=(
            pltpu.VMEM((NX, 32, 128), bf16),
            pltpu.VMEM((NB * NH, 128, 128), f32),
        ),
        in_specs=[anywhere] * 17,
        out_specs=(vmem, vmem),
        scratch_shapes=scratch,
        compiler_params=pltpu.CompilerParams(collective_id=0, has_side_effects=True),
        name="step",
    )(*operands)


def to_hbm(mixed, carried):
    parts = 4

    def body(mixed, carried, mixed_out, carried_out, sems):
        size = carried.shape[0] // parts
        copies = [pltpu.make_async_copy(mixed, mixed_out, sems.at[parts])]
        for i in range(parts):
            rows = pl.ds(i * size, size)
            copies.append(pltpu.make_async_copy(carried.at[rows], carried_out.at[rows], sems.at[i]))
        for copy in copies:
            copy.start()
        for copy in copies:
            copy.wait()

    vmem, hbm = pl.BlockSpec(memory_space=pltpu.VMEM), pl.BlockSpec(memory_space=pltpu.HBM)
    return pl.pallas_call(
        body,
        out_shape=tuple(pltpu.HBM(a.shape, a.dtype) for a in (mixed, carried)),
        in_specs=[vmem, vmem],
        out_specs=(hbm, hbm),
        scratch_shapes=[pltpu.SemaphoreType.DMA((parts + 1,))],
        name="to_hbm",
    )(pltpu.with_memory_space_constraint(mixed, pltpu.VMEM), pltpu.with_memory_space_constraint(carried, pltpu.VMEM))


def per_device(
    tokens,
    norm_gain,
    w_query,
    w_key,
    w_value,
    w_gate,
    w_decay,
    w_beta,
    decay_rate,
    head_gain,
    w_out,
    state,
    prev_keys,
    prev_values,
    prev_log_decay,
    prev_beta,
    accepted,
):
    mixed, carried = fused(
        tokens.reshape(NZ, NX, 32, 128), w_key, w_query, w_value, w_gate, w_out,
        state.reshape(NB * NH, 128, 128), norm_gain.reshape(NX * NZ, 128), w_decay.T, w_beta.T,
        prev_keys.reshape(128, 128), prev_values.reshape(128, 128),
        prev_log_decay.transpose(1, 2, 0).reshape(16, NB), prev_beta.transpose(1, 2, 0).reshape(16, NB),
        accepted.reshape(1, NB), decay_rate.reshape(1, 32), head_gain.reshape(1, 128),
    )
    mixed, carried = to_hbm(mixed, carried)
    return mixed.reshape(32, NT, 128), carried.reshape(NB, NH, 128, 128)


def solution(mesh):
    placed = (
        P(None, None, "kv"),
        P(),
        P("kv", "tp"),
        P("kv", "tp"),
        P("kv", "tp"),
        P("kv", "tp"),
        P(),
        P(),
        P(),
        P(),
        P("tp", "kv"),
        P("kv", "tp", None, None),
        P("kv", "tp", None, None),
        P("kv", "tp", None, None),
        P("kv", "tp", None),
        P("kv", "tp", None),
        P("kv"),
    )
    return jax.shard_map(
        per_device,
        mesh=mesh,
        in_specs=placed,
        out_specs=(P("tp", None, "kv"), P("kv", "tp", None, None)),
        check_vma=False,
    )
```
